32 devices in a mesh: sp: 4 (over x, core), tp: 8 (over z, y).
Axes of the slice: x: 2, y: 2, z: 4, core: 2. Of those that a mesh axis runs over, the one named last changes fastest.
Arguments:
- latents: bfloat16 [1024, 2048], P(('sp', 'tp')), may hold values from -6 to 6
- context: bfloat16 [256, 2048], P('sp'), may hold values from -6 to 6
- condition: float32 [2048], P('sp'), may hold values from -12 to 12
- context_condition: float32 [2048], P('sp'), may hold values from -12 to 12
- norm_gain: float32 [2048], replicated, may hold values from 0.1 to 1.9
- shift_weight: bfloat16 [2048, 2048], P('sp', 'tp'), may hold values from -0.09375 to 0.09375
- scale_weight: bfloat16 [2048, 2048], P('sp', 'tp'), may hold values from -0.09375 to 0.09375
- gate_weight: bfloat16 [2048, 2048], P('sp', 'tp'), may hold values from -0.125 to 0.125
- query_weight: bfloat16 [2048, 1024], P(None, 'tp'), may hold values from -0.125 to 0.125
- key_weight: bfloat16 [2048, 1024], P(None, 'tp'), may hold values from -0.125 to 0.125
- value_weight: bfloat16 [2048, 1024], P(None, 'tp'), may hold values from -0.125 to 0.125
- subtract_share: float32 [8], P('tp'), may hold values from 0.3 to 0.8
- head_gain: float32 [128], replicated, may hold values from 0.1 to 1.9
- output_weight: bfloat16 [1024, 2048], P('tp'), may hold values from -0.1875 to 0.1875
Outputs:
- updated: bfloat16 [1024, 2048], P(('sp', 'tp'))
The draws below stay inside these ranges and needn't reach their ends.
All inputs are finite; a program needn't handle non-finite values.
Results may differ from the reference program's by a relative error of at most 0.013.
Values may be sent and summed in bfloat16 or wider, within the bound.
A program may use at most 64 MiB of HBM per device.

```python
import math
import jax
import jax.numpy as jnp
from jax import lax

D = 2048
HEAD = 64
VALUE = 128
HEADS = 8
GRID_W = 64
TOKENS = 1024
CTX = 256


def ramped_draw(base_key):
    position = jnp.arange(D, dtype=jnp.float32) / (D - 1)
    values = jnp.clip(jax.random.normal(base_key, (D,), jnp.float32), -4.0, 4.0)
    growth = jnp.exp(jnp.log(3.0) * position)
    return values * growth


def draw_condition(key, part):
    return ramped_draw(jax.random.fold_in(key, 11))


def draw_context_condition(key, part):
    return ramped_draw(jax.random.fold_in(key, 29))


def block_levels(key, shape, cuts, least, largest):
    def one(dim, shards_of):
        heights = jax.random.uniform(jax.random.fold_in(jax.random.fold_in(key, 6), dim), (shards_of,), jnp.float32, least / len(cuts), largest / len(cuts))
        return jnp.repeat(jnp.exp(heights), shape[dim] // shards_of).reshape((-1,) + (1,) * (len(shape) - dim - 1))

    level = one(*cuts[0])
    for cut in cuts[1:]:
        level = level * one(*cut)
    return level


def centred(rng, dims, spread, limit, cuts=(), kind=jnp.bfloat16):
    array = spread * jax.random.normal(rng, dims, jnp.float32)
    if cuts:
        array = array * block_levels(rng, dims, cuts, -0.22, 0.18)
    return jnp.clip(array, -limit, limit).astype(kind)


def setup_inputs(seed: int = 0) -> dict:
    streams_of = jax.random.split(jax.random.key(seed), 15)
    latents = centred(streams_of[0], (TOKENS, D), 1.0, 6.0, ((0, 32),))
    context = centred(streams_of[1], (CTX, D), 1.0, 6.0, ((0, 4),))
    condition = draw_condition(jax.random.fold_in(streams_of[14], 71), 0)
    context_condition = draw_context_condition(jax.random.fold_in(streams_of[14], 71), 0)
    norm_gain = jnp.clip(1.0 + 0.18 * jax.random.normal(streams_of[4], (D,), jnp.float32), 0.1, 1.9)
    shift_weight = centred(streams_of[5], (D, D), (2 * D) ** -0.5, 0.09375, ((0, 4), (1, 8)))
    scale_weight = centred(streams_of[6], (D, D), (2 * D) ** -0.5, 0.09375, ((0, 4), (1, 8)))
    gate_weight = centred(streams_of[7], (D, D), D ** -0.5, 0.125, ((0, 4), (1, 8)))
    query_weight = centred(streams_of[8], (D, HEADS * VALUE), D ** -0.5, 0.125, ((1, 8),))
    key_weight = centred(streams_of[9], (D, HEADS * VALUE), D ** -0.5, 0.125, ((1, 8),))
    value_weight = centred(streams_of[10], (D, HEADS * VALUE), D ** -0.5, 0.125, ((1, 8),))
    subtract_share = jnp.clip(0.3 + 0.5 * jax.random.uniform(streams_of[11], (HEADS,), jnp.float32) ** block_levels(streams_of[11], (HEADS,), ((0, 8),), -0.2, 0.2), 0.3, 0.8)
    head_gain = jnp.clip(1.0 + 0.18 * jax.random.normal(streams_of[12], (VALUE,), jnp.float32), 0.1, 1.9)
    output_weight = centred(streams_of[13], (HEADS * VALUE, D), (HEADS * VALUE) ** -0.5, 0.1875, ((0, 8),))
    return dict(latents=latents, context=context, condition=condition, context_condition=context_condition, norm_gain=norm_gain, shift_weight=shift_weight, scale_weight=scale_weight, gate_weight=gate_weight, query_weight=query_weight, key_weight=key_weight, value_weight=value_weight, subtract_share=subtract_share, head_gain=head_gain, output_weight=output_weight)


norm_eps = 1e-06
head_eps = 1e-05
rope_theta = 10000.0
head_scale = 0.8

def rotary_tables(positions):
    quarter = HEAD // 4
    inverse = rope_theta ** (-2.0 * jnp.arange(quarter, dtype=jnp.float32) / (HEAD // 2))
    row_angle = (positions // GRID_W).astype(jnp.float32)[:, None] * inverse[None, :]
    column_angle = (positions % GRID_W).astype(jnp.float32)[:, None] * inverse[None, :]
    angles = jnp.concatenate([row_angle, row_angle, column_angle, column_angle], axis=-1)
    return (jnp.cos(angles), jnp.sin(angles))

def rotate(vectors, cosine, sine_table):
    quarter = HEAD // 4
    pieces = vectors.reshape(vectors.shape[:-1] + (2, 2, quarter))
    turned = jnp.concatenate([-pieces[..., 1:, :], pieces[..., :1, :]], axis=-2).reshape(vectors.shape)
    return vectors * cosine[:, None, :] + turned * sine_table[:, None, :]

def modulate(token_rows, gain_row, shift_row, scale_row):
    widened = token_rows.astype(jnp.float32)
    normed = widened * lax.rsqrt(lax.optimization_barrier(jnp.mean(widened * widened, axis=-1, keepdims=True)) + norm_eps)
    return (normed * gain_row * (1.0 + scale_row) + shift_row).astype(jnp.bfloat16)

def differential(queries, key_value_rows, share_value, head_gain):
    ratios = []
    for which_map in range(2):
        offset = which_map * HEAD
        scores = jnp.dot(queries[:, offset:offset + HEAD], key_value_rows[:, offset:offset + HEAD].T, preferred_element_type=jnp.float32) * HEAD ** (-0.5)
        powers = jnp.exp(scores)
        weighted = jnp.dot(powers.astype(jnp.bfloat16), key_value_rows[:, VALUE:], preferred_element_type=jnp.float32)
        ratios.append(weighted / lax.optimization_barrier(jnp.sum(powers, axis=1, keepdims=True)))
    difference = ratios[0] - share_value * ratios[1]
    normed = difference * lax.rsqrt(lax.optimization_barrier(jnp.mean(difference * difference, axis=1, keepdims=True)) + head_eps)
    return (normed * head_gain * head_scale).astype(jnp.bfloat16)

def reference(latents, context, condition, context_condition, norm_gain, shift_weight, scale_weight, gate_weight, query_weight, key_weight, value_weight, subtract_share, head_gain, output_weight):
    activated = jax.nn.silu(jnp.stack([condition, context_condition])).astype(jnp.bfloat16)
    shift_terms = jnp.dot(activated, shift_weight, preferred_element_type=jnp.float32)
    scale_terms = jnp.dot(activated, scale_weight, preferred_element_type=jnp.float32)
    gate_terms = jnp.dot(activated, gate_weight, preferred_element_type=jnp.float32)
    latent_mod = modulate(latents, norm_gain, shift_terms[0], scale_terms[0])
    context_mod = modulate(context, norm_gain, shift_terms[1], scale_terms[1])
    cosine, sine_table = rotary_tables(jnp.arange(TOKENS, dtype=jnp.int32))
    block_rows = math.gcd(TOKENS, 512)

    def add_head(head_index, running):
        first_column = jnp.asarray(head_index, jnp.int32) * VALUE

        def columns(weight):
            return lax.dynamic_slice_in_dim(weight, first_column, VALUE, 1)
        latent_query = jnp.dot(latent_mod, columns(query_weight), preferred_element_type=jnp.float32)
        queries = rotate(latent_query.reshape(TOKENS, 2, HEAD), cosine, sine_table)
        queries = queries.reshape(TOKENS, VALUE).astype(jnp.bfloat16)
        latent_key = jnp.dot(latent_mod, columns(key_weight), preferred_element_type=jnp.float32)
        latent_keys = rotate(latent_key.reshape(TOKENS, 2, HEAD), cosine, sine_table)
        latent_keys = latent_keys.reshape(TOKENS, VALUE).astype(jnp.bfloat16)
        latent_values = jnp.dot(latent_mod, columns(value_weight), preferred_element_type=jnp.float32).astype(jnp.bfloat16)
        context_keys = jnp.dot(context_mod, columns(key_weight), preferred_element_type=jnp.float32).astype(jnp.bfloat16)
        context_values = jnp.dot(context_mod, columns(value_weight), preferred_element_type=jnp.float32).astype(jnp.bfloat16)
        key_value_rows = jnp.concatenate([jnp.concatenate([context_keys, context_values], axis=1), jnp.concatenate([latent_keys, latent_values], axis=1)], axis=0)
        share_value = lax.dynamic_index_in_dim(subtract_share, jnp.asarray(head_index, jnp.int32), 0, keepdims=False)

        def one_block(query_block):
            return differential(query_block, key_value_rows, share_value, head_gain)
        head_output = lax.map(one_block, queries.reshape(TOKENS // block_rows, block_rows, VALUE))
        head_output = head_output.reshape(TOKENS, VALUE)
        output_rows = lax.dynamic_slice_in_dim(output_weight, first_column, VALUE, 0)
        return running + jnp.dot(head_output, output_rows, preferred_element_type=jnp.float32)
    branch = lax.fori_loop(0, HEADS, add_head, jnp.zeros((TOKENS, D), jnp.float32))
    return (latents.astype(jnp.float32) + gate_terms[0] * branch).astype(jnp.bfloat16)
```

```python
import functools
import math

import jax
import jax.numpy as jnp
from jax import lax
from jax.experimental import pallas as pl
from jax.experimental.pallas import tpu as pltpu
from jax.sharding import PartitionSpec as P

HEAD = 64
VALUE = 128
GRID_W = 64


norm_eps = 1e-06
head_eps = 1e-05
rope_theta = 10000.0
head_scale = 0.8


def rotary_tables(positions):
    quarter = HEAD // 4
    inverse = rope_theta ** (-2.0 * jnp.arange(quarter, dtype=jnp.float32) / (HEAD // 2))
    row_angle = (positions // GRID_W).astype(jnp.float32)[:, None] * inverse[None, :]
    column_angle = (positions % GRID_W).astype(jnp.float32)[:, None] * inverse[None, :]
    angles = jnp.concatenate([row_angle, row_angle, column_angle, column_angle], axis=-1)
    return (jnp.cos(angles), jnp.sin(angles))


def rotate(vectors, cosine, sine_table):
    quarter = HEAD // 4
    pieces = vectors.reshape(vectors.shape[:-1] + (2, 2, quarter))
    turned = jnp.concatenate([-pieces[..., 1:, :], pieces[..., :1, :]], axis=-2).reshape(
        vectors.shape
    )
    return vectors * cosine[:, None, :] + turned * sine_table[:, None, :]


def modulate(token_rows, gain_row, shift_row, scale_row):
    widened = token_rows.astype(jnp.float32)
    normed = widened * lax.rsqrt(jnp.mean(widened * widened, axis=-1, keepdims=True) + norm_eps)
    return (normed * gain_row * (1.0 + scale_row) + shift_row).astype(jnp.bfloat16)


def shards(
    latents,
    context,
    condition,
    context_condition,
    norm_gain,
    shift_weight,
    scale_weight,
    gate_weight,
    query_weight,
    key_weight,
    value_weight,
    subtract_share,
    head_gain,
    output_weight,
):
    activated = jax.nn.silu(jnp.stack([condition, context_condition])).astype(jnp.bfloat16)
    partial_terms = jnp.stack(
        [
            jnp.dot(activated, matrix, preferred_element_type=jnp.float32)
            for matrix in (shift_weight, scale_weight, gate_weight)
        ]
    )
    summed = lax.psum(partial_terms, "sp")
    full_terms = lax.all_gather(summed, "tp", axis=2, tiled=True)
    shift_terms, scale_terms, gate_terms = (full_terms[0], full_terms[1], full_terms[2])
    pair_weight = jnp.concatenate([key_weight, value_weight], axis=1)
    joined = jnp.concatenate([query_weight, pair_weight], axis=1)
    projected = jnp.dot(
        modulate(
            lax.all_gather(latents, "tp", axis=0, tiled=True),
            norm_gain,
            shift_terms[0],
            scale_terms[0],
        ),
        joined,
        preferred_element_type=jnp.float32,
    )
    local_count = projected.shape[0]
    positions = lax.axis_index("sp") * local_count + jnp.arange(local_count, dtype=jnp.int32)
    cosine, sine_table = rotary_tables(positions)
    queries = rotate(projected[:, :VALUE].reshape(local_count, 2, HEAD), cosine, sine_table)
    queries = queries.reshape(local_count, VALUE).astype(jnp.bfloat16)
    latent_keys = rotate(
        projected[:, VALUE : 2 * VALUE].reshape(local_count, 2, HEAD), cosine, sine_table
    )
    latent_keys = latent_keys.reshape(local_count, VALUE).astype(jnp.bfloat16)
    latent_pairs = jnp.concatenate(
        [latent_keys, projected[:, 2 * VALUE :].astype(jnp.bfloat16)], axis=1
    )
    context_mod = modulate(context, norm_gain, shift_terms[1], scale_terms[1])
    context_pairs = jnp.dot(context_mod, pair_weight, preferred_element_type=jnp.float32).astype(
        jnp.bfloat16
    )
    sent_pairs = jnp.concatenate([latent_pairs, context_pairs], axis=0)
    arrived = lax.all_gather(sent_pairs, "sp", axis=0, tiled=True)
    updated_carry = []
    for which_map in range(2):
        offset = which_map * HEAD
        scores = jnp.einsum(
            "qd,kd->qk",
            queries[:, offset : offset + HEAD],
            arrived[:, offset : offset + HEAD],
            preferred_element_type=jnp.float32,
        ) * HEAD ** (-0.5)
        powers = jnp.exp(scores)
        updated_carry.append(
            jnp.dot(
                powers.astype(jnp.bfloat16), arrived[:, VALUE:], preferred_element_type=jnp.float32
            )
        )
        updated_carry.append(jnp.sum(powers, axis=1, keepdims=True))
    first_sum, first_total, second_sum, second_total = tuple(updated_carry)
    share_value = subtract_share[0]
    difference = first_sum / first_total - share_value * (second_sum / second_total)
    normed = difference * lax.rsqrt(
        jnp.mean(difference * difference, axis=1, keepdims=True) + head_eps
    )
    head_output = (normed * head_gain * head_scale).astype(jnp.bfloat16)
    branch = lax.psum_scatter(
        jnp.dot(head_output, output_weight, preferred_element_type=jnp.float32),
        "tp",
        scatter_dimension=0,
        tiled=True,
    )
    return (latents.astype(jnp.float32) + gate_terms[0] * branch).astype(jnp.bfloat16)


MESH = pl.DeviceIdType.MESH
CHUNKS = 4
FAR_PIECES = 2
VMEM_LIMIT = 56 * 1024 * 1024


def fused_kernel(
    lat_hbm, ctx_hbm, cond_hbm, ccond_hbm, gain_hbm, shift_hbm, scale_hbm, gate_hbm,
    wq_hbm, wk_hbm, wv_hbm, share_hbm, hgain_hbm, wo_hbm, out_ref,
    ctx_ref, cond_ref, ccond_ref, gain_ref, share_ref, hgain_ref, lat, mod, cmod, wqkv, wo, wo_own,
    part, terms, tables, queries, kv, ho_send, ho, shift_ref, scale_ref, gate_ref, far_send, far_recv,
    load_sem, lat_ss, lat_rs, lat_xrs, lat_yss, lat_yrs, part_ss, part_rs, term_ss, term_rs, chain_sem,
    kv_ss, kv_rs, ckv_ss, ckv_rs, ho_ss, ho_rs, wo_mss, wo_ss, wo_rs, wo_xss, wo_xrs, wo_tss, wo_trs,
    far_ss, far_rs,
    *, S, T,
):
    f32, bf16 = jnp.float32, jnp.bfloat16
    count, D = lat.shape
    rows = count // T
    crows = ctx_ref.shape[0]
    width = D // T
    half = D // 2
    strip = half // S
    Z = T // 2
    i = lax.axis_index("sp")
    t = lax.axis_index("tp")
    z = lax.div(t, 2)
    y = lax.rem(t, 2)
    mate = t + 1 - 2 * y
    twin = i + 1 - 2 * lax.rem(i, 2)
    across = lax.rem(i + 2, S)
    twin_across = lax.rem(twin + 2, S)
    inner = jnp.logical_and(z > 0, z < Z - 1)
    outer = jnp.logical_or(z == 0, z == Z - 1)
    pending = []

    def when(cond, action):
        if cond is None:
            action()
        else:
            pl.when(cond)(action)

    def copy(src, dst, ss, rs, sp, tp):
        return pltpu.make_async_remote_copy(
            src_ref=src, dst_ref=dst, send_sem=ss, recv_sem=rs,
            device_id={"sp": sp, "tp": tp}, device_id_type=MESH,
        )

    def send(cond, src, dst, ss, rs, sp, tp, tracked=True):
        made = copy(src, dst, ss, rs, sp, tp)

        def go():
            made.start()

        when(cond, go)
        if tracked:
            pending.append((cond, made))

    def drain():
        for cond, made in pending:
            def finish(made=made):
                made.wait_send()

            when(cond, finish)
        pending.clear()

    def sent_all(view, ss):
        copy(view, view, ss, ss, twin, t).wait_send()

    def arrived(dst, ss, rs):
        copy(dst, dst, ss, rs, twin, t).wait_recv()

    def load(k, src, dst):
        return pltpu.make_async_copy(src, dst, load_sem.at[k])

    def half_cols(which):
        return pl.ds(pl.multiple_of(which * half, half), half)

    def strip_cols(which, share):
        return pl.ds(pl.multiple_of(which * half + share * strip, strip), strip)

    own_rows = pl.ds(pl.multiple_of(t * rows, rows), rows)
    own_load = load(0, lat_hbm, lat.at[own_rows, :])
    cond_loads = [load(1, cond_hbm, cond_ref), load(2, ccond_hbm, ccond_ref)]
    term_loads = [
        load(3, shift_hbm, shift_ref), load(4, scale_hbm, scale_ref), load(5, gate_hbm, gate_ref)
    ]
    qkv_loads = [
        load(6, wq_hbm, wqkv.at[:, pl.ds(0, VALUE)]),
        load(7, wk_hbm, wqkv.at[:, pl.ds(VALUE, VALUE)]),
        load(8, wv_hbm, wqkv.at[:, pl.ds(2 * VALUE, VALUE)]),
        load(9, ctx_hbm, ctx_ref),
        load(10, gain_hbm, gain_ref),
        load(11, share_hbm, share_ref),
        load(12, hgain_hbm, hgain_ref),
    ]
    wo_strip = load(13, wo_hbm.at[:, strip_cols(1 - y, i)], wo_own)
    wo_half = load(15, wo_hbm.at[:, half_cols(y)], wo.at[pl.ds(t * VALUE, VALUE), :])

    barrier = pltpu.get_barrier_semaphore()

    def greet(cond, sp, tp):
        def go():
            pl.semaphore_signal(
                barrier, inc=1, device_id={"sp": sp, "tp": tp}, device_id_type=MESH
            )

        when(cond, go)

    greet(z > 0, i, t - 2)
    greet(z < Z - 1, i, t + 2)
    greet(None, i, mate)
    for peer in (across, twin_across, twin):
        greet(None, peer, t)
    for made in [own_load] + cond_loads + term_loads + [wo_strip, wo_half] + qkv_loads:
        made.start()
    pl.semaphore_wait(
        barrier, 4 + (z > 0).astype(jnp.int32) + (z < Z - 1).astype(jnp.int32)
    )
    def chain(cond, which, tp):
        def go():
            pl.semaphore_signal(
                chain_sem.at[which], inc=1, device_id={"sp": i, "tp": tp}, device_id_type=MESH
            )

        when(cond, go)

    def chained(cond, which):
        def go():
            pl.semaphore_wait(chain_sem.at[which], 1)

        when(cond, go)

    below = z < Z - 1 - z
    inward = jnp.where(below, t + 4, t - 4)
    midward = jnp.where(below, t + 2, t - 2)
    outward = jnp.where(below, t - 2, t + 2)
    chain(inner, 0, outward)
    chain(outer, 1, midward)
    own_load.wait()

    step = D // CHUNKS

    def lat_piece(block, c):
        return lat.at[pl.ds(pl.multiple_of(block * rows, rows), rows), pl.ds(c * step, step)]

    def wo_piece(head, share):
        return wo.at[
            pl.ds(pl.multiple_of(head * VALUE, VALUE), VALUE),
            pl.ds(pl.multiple_of(share * strip, strip), strip),
        ]

    upper = range(CHUNKS // 2, CHUNKS)
    for c in range(CHUNKS):
        own = lat_piece(t, c)
        send(z < Z - 1, own, own, lat_ss.at[c, 0], lat_rs.at[c, z], i, t + 2)
        send(z > 0, own, own, lat_ss.at[c, 1], lat_rs.at[c, z], i, t - 2)
        rs = lat_rs.at[c, Z] if c in upper else lat_yrs.at[0]
        send(None, own, own, lat_yss.at[0], rs, i, mate, False)

    wo_strip.wait()
    send(None, wo_own, wo_piece(t, i), wo_mss.at[0], wo_rs.at[t], i, mate, False)

    def lat_far():
        for c in range(CHUNKS):
            own = lat_piece(t, c)
            send(outer, own, own, lat_ss.at[c, 2], lat_rs.at[c, z], i, inward)

    def lat_cross():
        for c in upper:
            piece = lat_piece(mate, c)
            arrived(piece, lat_yss.at[0], lat_rs.at[c, Z])
            send(outer, piece, piece, lat_ss.at[c, 3], lat_xrs.at[c], i, inward)

    def lat_stage(d, chunks=range(CHUNKS)):
        for c in chunks:
            for sign in (-1, 1):
                block = t + 2 * d * sign
                here = z - d >= 0 if sign < 0 else z + d < Z
                piece = lat_piece(block, c)
                layer = z + d * sign
                rs = lat_rs.at[c, layer]

                def come(piece=piece, rs=rs):
                    arrived(piece, lat_yss.at[0], rs)

                when(here, come)
                if d < Z - 1:
                    onward = jnp.logical_and(here, jnp.logical_and(inner, below == (sign > 0)))
                    send(onward, piece, piece, lat_ss.at[c, 1 + d], rs, i, outward)
                over = here
                if d > 1 and c in upper:
                    over = jnp.logical_and(here, outer)
                if d < Z - 1 or c not in upper:
                    send(over, piece, piece, lat_yss.at[0], lat_yrs.at[0], i, mate, False)

    def lat_last():
        opposite = 2 * (Z - 1 - z) + 1 - y
        for c in upper:
            for where, block in ((outer, opposite), (inner, mate + inward - t)):
                piece = lat_piece(block, c)

                def come(piece=piece, c=c):
                    arrived(piece, lat_yss.at[0], lat_xrs.at[c])

                when(where, come)
                if where is inner:
                    send(inner, piece, piece, lat_ss.at[c, 4], lat_xrs.at[c], i, outward)

    def wo_launch(cond, head, tp):
        piece = wo_piece(head, i)
        send(cond, piece, piece, wo_ss.at[0], wo_rs.at[head], i, tp, False)

    def wo_heads(d, sign):
        layer = 2 * (z + d * sign)
        return (layer + y, layer + 1 - y)

    def wo_take(cond, head, spread=True, onward=None):
        def go():
            piece = wo_piece(head, i)
            arrived(piece, wo_ss.at[0], wo_rs.at[head])

        def share():
            piece = wo_piece(head, i)
            copy(piece, piece, wo_xss.at[0], wo_xrs.at[head], across, t).start()
            copy(piece, piece, wo_tss.at[0], wo_trs.at[0], twin, t).start()

        when(cond, go)
        if onward is not None:
            wo_launch(onward, head, outward)
        if spread:
            when(cond, share)

    def wo_stage(d, where, middle=None):
        for sign in (-1, 1):
            here = z - d >= 0 if sign < 0 else z + d < Z
            here = jnp.logical_and(here, where)
            if middle is not None:
                here = jnp.logical_and(here, (below == (sign > 0)) == middle)
            onward = None
            if d < Z - 1:
                onward = jnp.logical_and(here, jnp.logical_and(inner, below == (sign > 0)))
            for head in wo_heads(d, sign):
                wo_take(here, head, True, onward)

    def wo_relay(d, where=None):
        todo = [(None, mate)] if d == 0 else [
            (z - d >= 0 if sign < 0 else z + d < Z, head)
            for sign in (-1, 1) for head in wo_heads(d, sign)
        ]
        for cond, head in todo:
            def go(head=head):
                piece = wo_piece(head, across)
                arrived(piece, wo_ss.at[0], wo_xrs.at[head])
                copy(piece, piece, wo_tss.at[0], wo_trs.at[0], twin, t).start()

            when(cond, go)

    def silu(v):
        return v / (1.0 + jnp.exp(-v))

    for made in cond_loads:
        made.wait()
    depth = cond_ref.shape[1]
    line = lax.broadcasted_iota(jnp.int32, (8, depth), 0)
    act0 = jnp.broadcast_to(silu(cond_ref[...]), (8, depth))
    act1 = jnp.broadcast_to(silu(ccond_ref[...]), (8, depth))

    def two_lines(first, matrix_ref, with_second):
        left = jnp.where(line == first, act0, 0.0)
        if with_second:
            left = jnp.where(line == first + 1, act1, left)
        return jnp.dot(left.astype(bf16), matrix_ref[...], preferred_element_type=f32)

    for made in term_loads:
        made.wait()
    part[pl.ds(i, 1)] = (
        two_lines(0, shift_ref, True) + two_lines(2, scale_ref, True) + two_lines(4, gate_ref, False)
    )[None]
    for k in range(1, S):
        send(None, part.at[i], part.at[i], part_ss.at[0], part_rs.at[0], lax.rem(i + k, S), t, False)

    lane = lax.broadcasted_iota(jnp.int32, (count, VALUE), 1)
    place = i * count + lax.broadcasted_iota(jnp.int32, (count, VALUE), 0)
    spot = lax.rem(lane, HEAD)
    quarter = HEAD // 4
    power = lax.rem(spot, quarter).astype(f32) * (-2.0 / (HEAD // 2))
    inverse = jnp.exp(power * math.log(rope_theta))
    along = jnp.where(spot < HEAD // 2, lax.div(place, GRID_W), lax.rem(place, GRID_W))
    angle = along.astype(f32) * inverse
    even = lax.rem(lax.div(spot, quarter), 2) == 0
    tables[0] = jnp.cos(angle)
    tables[1] = jnp.sin(angle)

    chained(outer, 0)
    lat_far()
    chained(inner, 1)
    chain(inner, 2, midward)
    chained(inner, 2)
    chain(inner, 2, outward)
    lat_stage(1, range(CHUNKS // 2))
    chained(outer, 2)

    arrived(part.at[pl.ds(0, S - 1)], part_ss.at[0], part_rs.at[0])
    total = part[0]
    for k in range(1, S):
        total = total + part[k]
    terms[pl.ds(t, 1)] = total[None]
    for k in range(1, T):
        send(
            None, terms.at[t], terms.at[t], term_ss.at[0], term_rs.at[0], i, lax.rem(t + k, T), False
        )

    lat_stage(1, range(CHUNKS // 2, CHUNKS))
    lat_cross()
    wo_half.wait()
    wo_take(None, mate)
    for head in (t, mate):
        wo_launch(None, head, midward)
    for d in range(2, Z):
        lat_stage(d)
        if d == 2:
            for head in (t, mate):
                wo_launch(outer, head, inward)
            wo_launch(inner, t, outward)
    lat_last()
    wo_launch(inner, mate, outward)
    wo_stage(1, inner, True)

    def modulate_into(dst, src, first, n, which):
        wide = src[...].astype(f32)
        factor = lax.rsqrt(jnp.mean(wide * wide, axis=-1, keepdims=True) + norm_eps)
        for j in range(T):
            cols = slice(j * width, (j + 1) * width)
            mult = gain_ref[:, cols] * (1.0 + terms[j, 2 + which : 3 + which, :])
            shifted = wide[:, cols] * factor * mult + terms[j, which : which + 1, :]
            dst[pl.ds(first, n), cols] = shifted.astype(bf16)

    for made in qkv_loads:
        made.wait()
    arrived(terms.at[pl.ds(0, T - 1)], term_ss.at[0], term_rs.at[0])
    modulate_into(cmod, ctx_ref, 0, crows, 1)
    kv[pl.ds(i, 1), pl.ds(count, crows), :] = jnp.dot(
        cmod[...], wqkv[:, VALUE:], preferred_element_type=f32
    ).astype(bf16)[None]

    def ckv_piece(s):
        return kv.at[s, pl.ds(count, crows), :]

    def kv_piece(s):
        return kv.at[s, pl.ds(0, count), :]

    send(None, ckv_piece(i), ckv_piece(i), ckv_ss.at[0], ckv_rs.at[i], across, t)
    send(None, ckv_piece(i), ckv_piece(i), ckv_ss.at[1], ckv_rs.at[i], twin, t)

    def over_view(where, less):
        return lat.at[pl.ds(0, Z * rows - rows + less), :]

    for where in (outer, inner):
        def come(where=where):
            arrived(over_view(where, 0), lat_yss.at[0], lat_yrs.at[0])

        when(where, come)
    modulate_into(mod, lat, 0, count, 0)
    projected = jnp.dot(mod[...], wqkv[...], preferred_element_type=f32)

    def rotated(u):
        turned = jnp.where(even, -pltpu.roll(u, VALUE - quarter, 1), pltpu.roll(u, quarter, 1))
        return u * tables[0] + turned * tables[1]

    kv[pl.ds(i, 1), pl.ds(0, count), pl.ds(0, VALUE)] = (
        rotated(projected[:, VALUE : 2 * VALUE]).astype(bf16)[None]
    )
    kv[pl.ds(i, 1), pl.ds(0, count), pl.ds(VALUE, VALUE)] = (
        projected[:, 2 * VALUE :].astype(bf16)[None]
    )
    send(None, kv_piece(i), kv_piece(i), kv_ss.at[0], kv_rs.at[i], across, t)
    send(None, kv_piece(i), kv_piece(i), kv_ss.at[1], kv_rs.at[i], twin, t)
    query = rotated(projected[:, :VALUE]).astype(bf16) * jnp.asarray(HEAD ** (-0.5), bf16)
    first_half = lane < HEAD
    zero = jnp.zeros_like(query)
    queries[0:count, :] = jnp.where(first_half, query, zero)
    queries[count:, :] = jnp.where(first_half, zero, query)

    ones = jnp.ones((count + crows, VALUE), bf16)

    def attend(slot):
        rows_kv = kv[slot]
        scores = lax.dot_general(
            queries[...], rows_kv[:, :VALUE], (((1,), (1,)), ((), ())), preferred_element_type=f32
        )
        return jnp.dot(
            jnp.exp(scores).astype(bf16),
            jnp.concatenate([rows_kv[:, VALUE:], ones], axis=1),
            preferred_element_type=f32,
        )

    sums = attend(i)
    arrived(ckv_piece(across), ckv_ss.at[2], ckv_rs.at[across])
    send(None, ckv_piece(across), ckv_piece(across), ckv_ss.at[2], ckv_rs.at[across], twin, t)
    wo_stage(2, inner)
    wo_relay(0)
    wo_stage(1, outer)
    arrived(kv_piece(twin), kv_ss.at[2], kv_rs.at[twin])
    arrived(ckv_piece(twin), ckv_ss.at[2], ckv_rs.at[twin])
    sums = sums + attend(twin)
    arrived(kv_piece(across), kv_ss.at[2], kv_rs.at[across])
    send(None, kv_piece(across), kv_piece(across), kv_ss.at[2], kv_rs.at[across], twin, t)
    wo_stage(1, inner, False)
    wo_stage(2, outer)
    sums = sums + attend(across)
    arrived(kv_piece(twin_across), kv_ss.at[2], kv_rs.at[twin_across])
    arrived(ckv_piece(twin_across), ckv_ss.at[2], ckv_rs.at[twin_across])
    sums = sums + attend(twin_across)
    ratio = sums[:, :VALUE] / sums[:, VALUE:]
    difference = ratio[:count] - share_ref[...] * ratio[count:]
    normed = difference * lax.rsqrt(
        jnp.mean(difference * difference, axis=1, keepdims=True) + head_eps
    )
    ho_send[...] = (normed * hgain_ref[...] * head_scale).astype(bf16)

    def pair_rows(layer):
        return ho_send.at[pl.ds(pl.multiple_of(layer * 2 * rows, 2 * rows), 2 * rows), :]

    for k in range(1, T):
        peer = lax.rem(t + k, T)
        send(None, pair_rows(lax.div(peer, 2)), ho.at[t], ho_ss.at[0], ho_rs.at[0], i, peer, False)
    ho[pl.ds(t, 1)] = pair_rows(z)[...][None]

    wo_stage(3, outer)
    wo_relay(1)
    wo_relay(2)
    wo_relay(3)
    drain()
    for where in (outer, inner):
        def left(where=where):
            sent_all(over_view(where, rows // 2), lat_yss.at[0])

        when(where, left)
    sent_all(part.at[pl.ds(0, S - 1)], part_ss.at[0])
    sent_all(terms.at[pl.ds(0, T - 1)], term_ss.at[0])
    other_rows = pl.ds(0, (T - 1) * VALUE)
    sent_all(wo_own, wo_mss.at[0])

    def wo_sent(heads):
        def go():
            sent_all(wo.at[pl.ds(0, heads * VALUE), pl.ds(0, strip)], wo_ss.at[0])

        return go

    when(outer, wo_sent(4))
    when(inner, wo_sent(8))
    arrived(wo.at[other_rows, pl.ds(0, 2 * strip)], wo_tss.at[0], wo_trs.at[0])
    arrived(ho.at[pl.ds(0, T - 1)], ho_ss.at[0], ho_rs.at[0])
    heads = jnp.concatenate(
        [
            jnp.concatenate(
                [ho[h, pl.ds(pl.multiple_of(which * rows, rows), rows), :] for h in range(T)], axis=1
            )
            for which in (1 - y, y)
        ],
        axis=0,
    )
    near = []
    blocks = T // 2
    per_piece = blocks // FAR_PIECES
    for j in range(blocks):
        gated = terms[pl.ds(y * blocks + j, 1), 4:5, :][0] * jnp.dot(
            heads, wo[:, j * width : (j + 1) * width], preferred_element_type=f32
        )
        far_send[:, j * width : (j + 1) * width] = gated[:rows].astype(bf16)
        near.append(gated[rows:])
        if (j + 1) % per_piece == 0:
            n = j // per_piece
            piece = pl.ds(n * per_piece * width, per_piece * width)
            send(
                None, far_send.at[:, piece], far_recv.at[:, piece], far_ss.at[n], far_rs.at[n], i, mate
            )
    for j in range(blocks):
        cols = pl.ds(pl.multiple_of(y * half + j * width, width), width)
        out_ref[:, cols] = (lat[own_rows, cols].astype(f32) + near[j]).astype(bf16)
    sent_all(wo.at[other_rows, pl.ds(0, strip)], wo_xss.at[0])
    sent_all(wo.at[other_rows, pl.ds(0, 2 * strip)], wo_tss.at[0])
    sent_all(ho.at[pl.ds(0, T - 1)], ho_ss.at[0])
    for n in range(FAR_PIECES):
        piece = pl.ds(n * per_piece * width, per_piece * width)
        arrived(far_recv.at[:, piece], far_ss.at[n], far_rs.at[n])
        for j in range(n * per_piece, (n + 1) * per_piece):
            cols = pl.ds(pl.multiple_of((1 - y) * half + j * width, width), width)
            out_ref[:, cols] = (
                lat[own_rows, cols].astype(f32)
                + far_recv[:, j * width : (j + 1) * width].astype(f32)
            ).astype(bf16)

    drain()


def fused_shards(S, T, *args):
    (latents, context, condition, context_condition, norm_gain, shift_weight, scale_weight,
     gate_weight, query_weight, key_weight, value_weight, subtract_share, head_gain,
     output_weight) = args
    rows, D = latents.shape
    crows = context.shape[0]
    count = rows * T
    Z = T // 2
    bf16, f32 = jnp.bfloat16, jnp.float32
    vmem = pl.BlockSpec(memory_space=pltpu.VMEM)
    hbm = pl.BlockSpec(memory_space=pltpu.HBM)
    dma = pltpu.SemaphoreType.DMA
    return pl.pallas_call(
        functools.partial(fused_kernel, S=S, T=T),
        out_shape=jax.ShapeDtypeStruct((rows, D), bf16),
        in_specs=[hbm] * 14,
        out_specs=vmem,
        scratch_shapes=[
            pltpu.VMEM((crows, D), bf16),
            pltpu.VMEM((1, condition.shape[0]), f32),
            pltpu.VMEM((1, condition.shape[0]), f32),
            pltpu.VMEM((1, D), f32),
            pltpu.VMEM((1, 1), f32),
            pltpu.VMEM((1, VALUE), f32),
            pltpu.VMEM((count, D), bf16),
            pltpu.VMEM((count, D), bf16),
            pltpu.VMEM((crows, D), bf16),
            pltpu.VMEM((D, 3 * VALUE), bf16),
            pltpu.VMEM((T * VALUE, D // 2), bf16),
            pltpu.VMEM((VALUE, D // (2 * S)), bf16),
            pltpu.VMEM((S, 8, D // T), f32),
            pltpu.VMEM((T, 8, D // T), f32),
            pltpu.VMEM((2, count, VALUE), f32),
            pltpu.VMEM((2 * count, VALUE), bf16),
            pltpu.VMEM((S, count + crows, 2 * VALUE), bf16),
            pltpu.VMEM((count, VALUE), bf16),
            pltpu.VMEM((T, 2 * rows, VALUE), bf16),
            pltpu.VMEM(shift_weight.shape, bf16),
            pltpu.VMEM(shift_weight.shape, bf16),
            pltpu.VMEM(shift_weight.shape, bf16),
            pltpu.VMEM((rows, D // 2), bf16),
            pltpu.VMEM((rows, D // 2), bf16),
            dma((16,)), dma((CHUNKS, 5)), dma((CHUNKS, Z + 1)), dma((CHUNKS,)), dma((1,)), dma((1,)),
            dma((1,)), dma((1,)), dma((1,)), dma((1,)), pltpu.SemaphoreType.REGULAR((3,)),
            dma((3,)), dma((S,)), dma((3,)), dma((S,)),
            dma((1,)), dma((1,)), dma((1,)), dma((1,)), dma((T,)), dma((1,)), dma((T,)), dma((1,)), dma((1,)),
            dma((FAR_PIECES,)), dma((FAR_PIECES,)),
        ],
        compiler_params=pltpu.CompilerParams(
            collective_id=0, has_side_effects=True, vmem_limit_bytes=VMEM_LIMIT
        ),
    )(latents, context, condition[None, :], context_condition[None, :], norm_gain[None, :],
      shift_weight, scale_weight, gate_weight, query_weight, key_weight, value_weight,
      subtract_share[None, :], head_gain[None, :], output_weight)


def fits(S, T, shapes):
    rows = shapes[0][0] // (S * T)
    crows = shapes[1][0] // S
    D = shapes[0][1]
    heads = shapes[8][1] // VALUE
    return (
        S == 4 and T == 8 and heads == T and rows % 32 == 0
        and crows % 16 == 0 and D % (128 * T) == 0 and D % (128 * CHUNKS) == 0
        and rows * T * D * 8 + T * VALUE * D * 2 < 24 * 1024 * 1024
    )


def solution(mesh):
    in_specs = (
        P(("sp", "tp"), None),
        P("sp", None),
        P("sp"),
        P("sp"),
        P(),
        P("sp", "tp"),
        P("sp", "tp"),
        P("sp", "tp"),
        P(None, "tp"),
        P(None, "tp"),
        P(None, "tp"),
        P("tp"),
        P(),
        P("tp", None),
    )
    out_specs = P(("sp", "tp"), None)
    S, T = mesh.shape["sp"], mesh.shape["tp"]

    def whole(*args):
        if fits(S, T, [a.shape for a in args]):
            body = functools.partial(fused_shards, S, T)
        else:
            body = shards
        return jax.shard_map(
            body, mesh=mesh, in_specs=in_specs, out_specs=out_specs, check_vma=False
        )(*args)

    return whole
```

```python
import functools
import math

import jax
import jax.numpy as jnp
from jax import lax
from jax.experimental import pallas as pl
from jax.experimental.pallas import tpu as pltpu
from jax.sharding import PartitionSpec as P

HEAD = 64
VALUE = 128
GRID_W = 64


norm_eps = 1e-06
head_eps = 1e-05
rope_theta = 10000.0
head_scale = 0.8


def rotary_tables(positions):
    quarter = HEAD // 4
    inverse = rope_theta ** (-2.0 * jnp.arange(quarter, dtype=jnp.float32) / (HEAD // 2))
    row_angle = (positions // GRID_W).astype(jnp.float32)[:, None] * inverse[None, :]
    column_angle = (positions % GRID_W).astype(jnp.float32)[:, None] * inverse[None, :]
    angles = jnp.concatenate([row_angle, row_angle, column_angle, column_angle], axis=-1)
    return (jnp.cos(angles), jnp.sin(angles))


def rotate(vectors, cosine, sine_table):
    quarter = HEAD // 4
    pieces = vectors.reshape(vectors.shape[:-1] + (2, 2, quarter))
    turned = jnp.concatenate([-pieces[..., 1:, :], pieces[..., :1, :]], axis=-2).reshape(
        vectors.shape
    )
    return vectors * cosine[:, None, :] + turned * sine_table[:, None, :]


def modulate(token_rows, gain_row, shift_row, scale_row):
    widened = token_rows.astype(jnp.float32)
    normed = widened * lax.rsqrt(jnp.mean(widened * widened, axis=-1, keepdims=True) + norm_eps)
    return (normed * gain_row * (1.0 + scale_row) + shift_row).astype(jnp.bfloat16)


def shards(
    latents,
    context,
    condition,
    context_condition,
    norm_gain,
    shift_weight,
    scale_weight,
    gate_weight,
    query_weight,
    key_weight,
    value_weight,
    subtract_share,
    head_gain,
    output_weight,
):
    activated = jax.nn.silu(jnp.stack([condition, context_condition])).astype(jnp.bfloat16)
    partial_terms = jnp.stack(
        [
            jnp.dot(activated, matrix, preferred_element_type=jnp.float32)
            for matrix in (shift_weight, scale_weight, gate_weight)
        ]
    )
    summed = lax.psum(partial_terms, "sp")
    full_terms = lax.all_gather(summed, "tp", axis=2, tiled=True)
    shift_terms, scale_terms, gate_terms = (full_terms[0], full_terms[1], full_terms[2])
    pair_weight = jnp.concatenate([key_weight, value_weight], axis=1)
    joined = jnp.concatenate([query_weight, pair_weight], axis=1)
    projected = jnp.dot(
        modulate(
            lax.all_gather(latents, "tp", axis=0, tiled=True),
            norm_gain,
            shift_terms[0],
            scale_terms[0],
        ),
        joined,
        preferred_element_type=jnp.float32,
    )
    local_count = projected.shape[0]
    positions = lax.axis_index("sp") * local_count + jnp.arange(local_count, dtype=jnp.int32)
    cosine, sine_table = rotary_tables(positions)
    queries = rotate(projected[:, :VALUE].reshape(local_count, 2, HEAD), cosine, sine_table)
    queries = queries.reshape(local_count, VALUE).astype(jnp.bfloat16)
    latent_keys = rotate(
        projected[:, VALUE : 2 * VALUE].reshape(local_count, 2, HEAD), cosine, sine_table
    )
    latent_keys = latent_keys.reshape(local_count, VALUE).astype(jnp.bfloat16)
    latent_pairs = jnp.concatenate(
        [latent_keys, projected[:, 2 * VALUE :].astype(jnp.bfloat16)], axis=1
    )
    context_mod = modulate(context, norm_gain, shift_terms[1], scale_terms[1])
    context_pairs = jnp.dot(context_mod, pair_weight, preferred_element_type=jnp.float32).astype(
        jnp.bfloat16
    )
    sent_pairs = jnp.concatenate([latent_pairs, context_pairs], axis=0)
    arrived = lax.all_gather(sent_pairs, "sp", axis=0, tiled=True)
    updated_carry = []
    for which_map in range(2):
        offset = which_map * HEAD
        scores = jnp.einsum(
            "qd,kd->qk",
            queries[:, offset : offset + HEAD],
            arrived[:, offset : offset + HEAD],
            preferred_element_type=jnp.float32,
        ) * HEAD ** (-0.5)
        powers = jnp.exp(scores)
        updated_carry.append(
            jnp.dot(
                powers.astype(jnp.bfloat16), arrived[:, VALUE:], preferred_element_type=jnp.float32
            )
        )
        updated_carry.append(jnp.sum(powers, axis=1, keepdims=True))
    first_sum, first_total, second_sum, second_total = tuple(updated_carry)
    share_value = subtract_share[0]
    difference = first_sum / first_total - share_value * (second_sum / second_total)
    normed = difference * lax.rsqrt(
        jnp.mean(difference * difference, axis=1, keepdims=True) + head_eps
    )
    head_output = (normed * head_gain * head_scale).astype(jnp.bfloat16)
    branch = lax.psum_scatter(
        jnp.dot(head_output, output_weight, preferred_element_type=jnp.float32),
        "tp",
        scatter_dimension=0,
        tiled=True,
    )
    return (latents.astype(jnp.float32) + gate_terms[0] * branch).astype(jnp.bfloat16)


MESH = pl.DeviceIdType.MESH
CHUNKS = 4
FAR_PIECES = 4
VMEM_LIMIT = 55000 * 1024


def fused_kernel(
    lat_hbm, ctx_hbm, cond_hbm, ccond_hbm, gain_hbm, shift_hbm, scale_hbm, gate_hbm,
    wq_hbm, wk_hbm, wv_hbm, share_hbm, hgain_hbm, wo_hbm, out_ref,
    ctx_ref, cond_ref, ccond_ref, gain_ref, share_ref, hgain_ref, lat, mod, cmod, wqkv, wo, wo_own,
    part, terms, tables, queries, kv, ho_send, ho, shift_ref, scale_ref, gate_ref, far_send, far_recv, acc,
    load_sem, lat_ss, lat_rs, lat_xrs, lat_yss, lat_yrs, part_ss, part_rs, term_ss, term_rs, chain_sem,
    kv_ss, kv_rs, ckv_ss, ckv_rs, ho_ss, ho_rs, wo_mss, wo_ss, wo_rs, wo_xss, wo_xrs, wo_tss, wo_trs,
    far_ss, far_rs,
    *, S, T,
):
    f32, bf16 = jnp.float32, jnp.bfloat16
    count, D = lat.shape
    rows = count // T
    crows = ctx_ref.shape[0]
    width = D // T
    half = D // 2
    strip = half // S
    Z = T // 2
    i = lax.axis_index("sp")
    t = lax.axis_index("tp")
    z = lax.div(t, 2)
    y = lax.rem(t, 2)
    mate = t + 1 - 2 * y
    twin = i + 1 - 2 * lax.rem(i, 2)
    across = lax.rem(i + 2, S)
    twin_across = lax.rem(twin + 2, S)
    inner = jnp.logical_and(z > 0, z < Z - 1)
    outer = jnp.logical_or(z == 0, z == Z - 1)
    pending = []

    def when(cond, action):
        if cond is None:
            action()
        else:
            pl.when(cond)(action)

    def copy(src, dst, ss, rs, sp, tp):
        return pltpu.make_async_remote_copy(
            src_ref=src, dst_ref=dst, send_sem=ss, recv_sem=rs,
            device_id={"sp": sp, "tp": tp}, device_id_type=MESH,
        )

    def send(cond, src, dst, ss, rs, sp, tp, tracked=True):
        made = copy(src, dst, ss, rs, sp, tp)

        def go():
            made.start()

        when(cond, go)
        if tracked:
            pending.append((cond, made))

    def drain():
        for cond, made in pending:
            def finish(made=made):
                made.wait_send()

            when(cond, finish)
        pending.clear()

    def sent_all(view, ss):
        copy(view, view, ss, ss, twin, t).wait_send()

    def arrived(dst, ss, rs):
        copy(dst, dst, ss, rs, twin, t).wait_recv()

    def load(k, src, dst):
        return pltpu.make_async_copy(src, dst, load_sem.at[k])

    def half_cols(which):
        return pl.ds(pl.multiple_of(which * half, half), half)

    def strip_cols(which, share):
        return pl.ds(pl.multiple_of(which * half + share * strip, strip), strip)

    own_rows = pl.ds(pl.multiple_of(t * rows, rows), rows)
    own_load = load(0, lat_hbm, lat.at[own_rows, :])
    cond_loads = [load(1, cond_hbm, cond_ref), load(2, ccond_hbm, ccond_ref)]
    term_loads = [
        load(3, shift_hbm, shift_ref), load(4, scale_hbm, scale_ref), load(5, gate_hbm, gate_ref)
    ]
    qkv_loads = [
        load(6, wq_hbm, wqkv.at[:, pl.ds(0, VALUE)]),
        load(7, wk_hbm, wqkv.at[:, pl.ds(VALUE, VALUE)]),
        load(8, wv_hbm, wqkv.at[:, pl.ds(2 * VALUE, VALUE)]),
        load(9, ctx_hbm, ctx_ref),
        load(10, gain_hbm, gain_ref),
        load(11, share_hbm, share_ref),
        load(12, hgain_hbm, hgain_ref),
    ]
    wo_strip = load(13, wo_hbm.at[:, strip_cols(1 - y, i)], wo_own)
    wo_half = load(15, wo_hbm.at[:, half_cols(y)], wo.at[pl.ds(t * VALUE, VALUE), :])

    barrier = pltpu.get_barrier_semaphore()

    def greet(cond, sp, tp):
        def go():
            pl.semaphore_signal(
                barrier, inc=1, device_id={"sp": sp, "tp": tp}, device_id_type=MESH
            )

        when(cond, go)

    greet(z > 0, i, t - 2)
    greet(z < Z - 1, i, t + 2)
    greet(None, i, mate)
    for peer in (across, twin_across, twin):
        greet(None, peer, t)
    for made in [own_load] + cond_loads + term_loads + [wo_strip, wo_half] + qkv_loads:
        made.start()
    pl.semaphore_wait(
        barrier, 4 + (z > 0).astype(jnp.int32) + (z < Z - 1).astype(jnp.int32)
    )
    def chain(cond, which, tp):
        def go():
            pl.semaphore_signal(
                chain_sem.at[which], inc=1, device_id={"sp": i, "tp": tp}, device_id_type=MESH
            )

        when(cond, go)

    def chained(cond, which):
        def go():
            pl.semaphore_wait(chain_sem.at[which], 1)

        when(cond, go)

    below = z < Z - 1 - z
    inward = jnp.where(below, t + 4, t - 4)
    midward = jnp.where(below, t + 2, t - 2)
    outward = jnp.where(below, t - 2, t + 2)
    chain(inner, 0, outward)
    chain(outer, 1, midward)
    own_load.wait()

    step = D // CHUNKS

    def lat_piece(block, c):
        return lat.at[pl.ds(pl.multiple_of(block * rows, rows), rows), pl.ds(c * step, step)]

    def wo_piece(head, share):
        return wo.at[
            pl.ds(pl.multiple_of(head * VALUE, VALUE), VALUE),
            pl.ds(pl.multiple_of(share * strip, strip), strip),
        ]

    upper = range(CHUNKS // 2, CHUNKS)
    for c in range(CHUNKS):
        own = lat_piece(t, c)
        send(z < Z - 1, own, own, lat_ss.at[c, 0], lat_rs.at[c, z], i, t + 2)
        send(z > 0, own, own, lat_ss.at[c, 1], lat_rs.at[c, z], i, t - 2)
        rs = lat_rs.at[c, Z] if c in upper else lat_yrs.at[0]
        send(None, own, own, lat_yss.at[0], rs, i, mate, False)

    wo_strip.wait()
    send(None, wo_own, wo_piece(t, i), wo_mss.at[0], wo_rs.at[t], i, mate, False)

    def lat_far():
        for c in range(CHUNKS):
            own = lat_piece(t, c)
            send(outer, own, own, lat_ss.at[c, 2], lat_rs.at[c, z], i, inward)

    opposite = 2 * (Z - 1 - z) + y

    def lat_cross():
        for c in upper:
            piece = lat_piece(mate, c)
            arrived(piece, lat_yss.at[0], lat_rs.at[c, Z])
            send(outer, piece, piece, lat_ss.at[c, 3], lat_xrs.at[c], i, opposite)

    def lat_stage(d, chunks=range(CHUNKS)):
        for c in chunks:
            for sign in (-1, 1):
                block = t + 2 * d * sign
                here = z - d >= 0 if sign < 0 else z + d < Z
                piece = lat_piece(block, c)
                layer = z + d * sign
                rs = lat_rs.at[c, layer]

                def come(piece=piece, rs=rs):
                    arrived(piece, lat_yss.at[0], rs)

                when(here, come)
                if d < Z - 1:
                    onward = jnp.logical_and(here, jnp.logical_and(inner, below == (sign > 0)))
                    send(onward, piece, piece, lat_ss.at[c, 1 + d], rs, i, outward)
                if d < Z - 1 or c not in upper:
                    batch = jnp.where((2 * layer < Z) == below, 0, 1)
                    send(here, piece, piece, lat_yss.at[0], lat_yrs.at[batch], i, mate, False)

    def lat_last():
        def come():
            for c in upper:
                arrived(lat_piece(opposite + mate - t, c), lat_yss.at[0], lat_xrs.at[c])

        when(outer, come)

    def wo_launch(cond, head, tp):
        piece = wo_piece(head, i)
        send(cond, piece, piece, wo_ss.at[0], wo_rs.at[head], i, tp, False)

    def wo_heads(d, sign):
        layer = 2 * (z + d * sign)
        return (layer + y, layer + 1 - y)

    def late_head(head):
        layer = lax.div(head, 2)
        return jnp.where(layer == jnp.where(below, Z - 1, 0), 1, 0)

    def wo_take(cond, head, onward=None):
        def go():
            piece = wo_piece(head, i)
            arrived(piece, wo_ss.at[0], wo_rs.at[head])

        when(cond, go)
        if onward is not None:
            wo_launch(onward, head, outward)

    def wo_share(cond, head):
        def go():
            piece = wo_piece(head, i)
            copy(piece, piece, wo_xss.at[0], wo_xrs.at[head], across, t).start()
            copy(piece, piece, wo_tss.at[0], wo_trs.at[late_head(head)], twin, t).start()

        when(cond, go)

    def wo_stage(d, where, middle=None, take=True, share=True):
        for sign in (-1, 1):
            here = z - d >= 0 if sign < 0 else z + d < Z
            here = jnp.logical_and(here, where)
            if middle is not None:
                here = jnp.logical_and(here, (below == (sign > 0)) == middle)
            onward = None
            if d < Z - 1:
                onward = jnp.logical_and(here, jnp.logical_and(inner, below == (sign > 0)))
            for head in wo_heads(d, sign):
                if take:
                    wo_take(here, head, onward)
                if share:
                    wo_share(here, head)

    def wo_relay(d, where=None):
        todo = [(None, mate)] if d == 0 else [
            (z - d >= 0 if sign < 0 else z + d < Z, head)
            for sign in (-1, 1) for head in wo_heads(d, sign)
        ]
        for cond, head in todo:
            def go(head=head):
                piece = wo_piece(head, across)
                arrived(piece, wo_ss.at[0], wo_xrs.at[head])
                copy(piece, piece, wo_tss.at[0], wo_trs.at[late_head(head)], twin, t).start()

            when(cond, go)

    def silu(v):
        return v / (1.0 + jnp.exp(-v))

    for made in cond_loads:
        made.wait()
    depth = cond_ref.shape[1]
    line = lax.broadcasted_iota(jnp.int32, (8, depth), 0)
    act0 = jnp.broadcast_to(silu(cond_ref[...]), (8, depth))
    act1 = jnp.broadcast_to(silu(ccond_ref[...]), (8, depth))

    def two_lines(first, matrix_ref, with_second):
        left = jnp.where(line == first, act0, 0.0)
        if with_second:
            left = jnp.where(line == first + 1, act1, left)
        return jnp.dot(left.astype(bf16), matrix_ref[...], preferred_element_type=f32)

    for made in term_loads:
        made.wait()
    part[pl.ds(i, 1)] = (
        two_lines(0, shift_ref, True) + two_lines(2, scale_ref, True) + two_lines(4, gate_ref, False)
    )[None]
    for k in range(1, S):
        send(None, part.at[i], part.at[i], part_ss.at[0], part_rs.at[0], lax.rem(i + k, S), t, False)

    lane = lax.broadcasted_iota(jnp.int32, (count, VALUE), 1)
    place = i * count + lax.broadcasted_iota(jnp.int32, (count, VALUE), 0)
    spot = lax.rem(lane, HEAD)
    quarter = HEAD // 4
    power = lax.rem(spot, quarter).astype(f32) * (-2.0 / (HEAD // 2))
    inverse = jnp.exp(power * math.log(rope_theta))
    along = jnp.where(spot < HEAD // 2, lax.div(place, GRID_W), lax.rem(place, GRID_W))
    angle = along.astype(f32) * inverse
    even = lax.rem(lax.div(spot, quarter), 2) == 0
    tables[0] = jnp.cos(angle)
    tables[1] = jnp.sin(angle)

    chained(outer, 0)
    lat_far()
    chained(inner, 1)
    chain(inner, 2, midward)
    chained(inner, 2)
    chain(inner, 2, outward)
    lat_stage(1, range(CHUNKS // 2))
    chained(outer, 2)

    arrived(part.at[pl.ds(0, S - 1)], part_ss.at[0], part_rs.at[0])
    total = part[0]
    for k in range(1, S):
        total = total + part[k]
    terms[pl.ds(t, 1)] = total[None]
    for k in range(1, T):
        send(
            None, terms.at[t], terms.at[t], term_ss.at[0], term_rs.at[0], i, lax.rem(t + k, T), False
        )

    lat_stage(1, range(CHUNKS // 2, CHUNKS))
    lat_cross()
    wo_half.wait()
    wo_take(None, mate)
    wo_share(None, mate)
    for head in (t, mate):
        wo_launch(None, head, midward)
        wo_launch(outer, head, inward)
    lat_stage(2)
    wo_launch(inner, t, outward)
    wo_launch(inner, mate, outward)
    lat_stage(3, range(CHUNKS // 2))

    def modulate_into(dst, src, first, n, which):
        wide = src[...].astype(f32)
        factor = lax.rsqrt(jnp.mean(wide * wide, axis=-1, keepdims=True) + norm_eps)
        for j in range(T):
            cols = slice(j * width, (j + 1) * width)
            mult = gain_ref[:, cols] * (1.0 + terms[j, 2 + which : 3 + which, :])
            shifted = wide[:, cols] * factor * mult + terms[j, which : which + 1, :]
            dst[pl.ds(first, n), cols] = shifted.astype(bf16)

    def ckv_piece(s):
        return kv.at[s, pl.ds(count, crows), :]

    part_rows = count // 2
    batch_first = [
        pl.multiple_of(jnp.where(below == (b == 0), 0, part_rows), part_rows) for b in range(2)
    ]

    def kv_piece(s, b):
        return kv.at[s, pl.ds(batch_first[b], part_rows), :]

    first_half = lax.broadcasted_iota(jnp.int32, (part_rows, VALUE), 1) < HEAD

    def project_batch(b):
        first = batch_first[b]
        which = pl.ds(first, part_rows)
        modulate_into(mod, lat.at[which, :], 0, part_rows, 0)
        projected = jnp.dot(mod[...], wqkv[...], preferred_element_type=f32)

        def rotated(u):
            turned = jnp.where(
                even[:part_rows], -pltpu.roll(u, VALUE - quarter, 1), pltpu.roll(u, quarter, 1)
            )
            return u * tables[0, which, :] + turned * tables[1, which, :]

        kv[pl.ds(i, 1), which, pl.ds(0, VALUE)] = (
            rotated(projected[:, VALUE : 2 * VALUE]).astype(bf16)[None]
        )
        kv[pl.ds(i, 1), which, pl.ds(VALUE, VALUE)] = projected[:, 2 * VALUE :].astype(bf16)[None]
        own = kv_piece(i, b)
        send(None, own, own, kv_ss.at[b, 0], kv_rs.at[b, i], across, t)
        send(None, own, own, kv_ss.at[b, 1], kv_rs.at[b, i], twin, t)
        query = rotated(projected[:, :VALUE]).astype(bf16) * jnp.asarray(HEAD ** (-0.5), bf16)
        zero = jnp.zeros_like(query)
        queries[which, :] = jnp.where(first_half, query, zero)
        queries[pl.ds(pl.multiple_of(count + first, part_rows), part_rows), :] = jnp.where(
            first_half, zero, query
        )

    def kv_relay(b):
        piece = kv_piece(across, b)
        arrived(piece, kv_ss.at[b, 2], kv_rs.at[b, across])
        send(None, piece, piece, kv_ss.at[b, 2], kv_rs.at[b, across], twin, t)

    for made in qkv_loads:
        made.wait()
    arrived(terms.at[pl.ds(0, T - 1)], term_ss.at[0], term_rs.at[0])
    modulate_into(cmod, ctx_ref, 0, crows, 1)
    kv[pl.ds(i, 1), pl.ds(count, crows), :] = jnp.dot(
        cmod[...], wqkv[:, VALUE:], preferred_element_type=f32
    ).astype(bf16)[None]
    send(None, ckv_piece(i), ckv_piece(i), ckv_ss.at[0], ckv_rs.at[i], across, t)
    send(None, ckv_piece(i), ckv_piece(i), ckv_ss.at[1], ckv_rs.at[i], twin, t)

    def over_wait(n, ss, rs):
        view = lat.at[pl.ds(0, n), :]
        if rs is None:
            sent_all(view, ss)
        else:
            arrived(view, ss, rs)

    over_wait(3 * rows // 2, lat_yss.at[0], lat_yrs.at[0])
    project_batch(0)
    lat_stage(3, upper)
    lat_last()
    wo_stage(1, inner, True, share=False)
    when(outer, lambda: over_wait(3 * rows // 2, lat_yss.at[0], lat_yrs.at[1]))
    when(inner, lambda: over_wait(2 * rows, lat_yss.at[0], lat_yrs.at[1]))
    project_batch(1)
    wo_stage(1, inner, True, take=False)
    wo_stage(2, inner)
    wo_stage(1, outer)
    arrived(ckv_piece(across), ckv_ss.at[2], ckv_rs.at[across])
    send(None, ckv_piece(across), ckv_piece(across), ckv_ss.at[2], ckv_rs.at[across], twin, t)
    kv_relay(0)

    def attend(rows_kv):
        scores = lax.dot_general(
            queries[...], rows_kv[:, :VALUE], (((1,), (1,)), ((), ())), preferred_element_type=f32
        )
        ones = jnp.ones((rows_kv.shape[0], VALUE), bf16)
        return jnp.dot(
            jnp.exp(scores).astype(bf16),
            jnp.concatenate([rows_kv[:, VALUE:], ones], axis=1),
            preferred_element_type=f32,
        )

    def attend_first(s):
        return attend(jnp.concatenate([kv_piece(s, 0)[...], ckv_piece(s)[...]], axis=0))

    sums = attend(kv[i])
    wo_relay(0)
    arrived(kv_piece(twin, 0), kv_ss.at[0, 2], kv_rs.at[0, twin])
    arrived(ckv_piece(twin), ckv_ss.at[2], ckv_rs.at[twin])
    sums = sums + attend_first(twin)
    sums = sums + attend_first(across)
    arrived(kv_piece(twin_across, 0), kv_ss.at[0, 2], kv_rs.at[0, twin_across])
    arrived(ckv_piece(twin_across), ckv_ss.at[2], ckv_rs.at[twin_across])
    sums = sums + attend_first(twin_across)
    wo_stage(1, inner, False)
    arrived(kv_piece(twin, 1), kv_ss.at[1, 2], kv_rs.at[1, twin])
    sums = sums + attend(kv_piece(twin, 1)[...])
    kv_relay(1)
    wo_stage(2, outer)
    sums = sums + attend(kv_piece(across, 1)[...])
    arrived(kv_piece(twin_across, 1), kv_ss.at[1, 2], kv_rs.at[1, twin_across])
    sums = sums + attend(kv_piece(twin_across, 1)[...])
    ratio = sums[:, :VALUE] / sums[:, VALUE:]
    difference = ratio[:count] - share_ref[...] * ratio[count:]
    normed = difference * lax.rsqrt(
        jnp.mean(difference * difference, axis=1, keepdims=True) + head_eps
    )
    ho_send[...] = (normed * hgain_ref[...] * head_scale).astype(bf16)

    def pair_rows(layer):
        return ho_send.at[pl.ds(pl.multiple_of(layer * 2 * rows, 2 * rows), 2 * rows), :]

    for k in range(1, T):
        peer = lax.rem(t + k, T)
        send(None, pair_rows(lax.div(peer, 2)), ho.at[t], ho_ss.at[0], ho_rs.at[0], i, peer, False)
    ho[pl.ds(t, 1)] = pair_rows(z)[...][None]

    wo_stage(3, outer)
    wo_relay(1)
    for where in (outer, inner):
        def second(where=where):
            if where is outer:
                wo_relay(2)

        when(where, second)
    drain()
    when(outer, lambda: over_wait(7 * rows // 2, lat_yss.at[0], None))
    when(inner, lambda: over_wait(4 * rows, lat_yss.at[0], None))
    sent_all(part.at[pl.ds(0, S - 1)], part_ss.at[0])
    sent_all(terms.at[pl.ds(0, T - 1)], term_ss.at[0])
    sent_all(wo_own, wo_mss.at[0])

    def wo_sent(heads):
        def go():
            sent_all(wo.at[pl.ds(0, heads * VALUE), pl.ds(0, strip)], wo_ss.at[0])

        return go

    when(outer, wo_sent(4))
    when(inner, wo_sent(8))
    early_heads = T - 3
    arrived(wo.at[pl.ds(0, early_heads * VALUE), pl.ds(0, 2 * strip)], wo_tss.at[0], wo_trs.at[0])
    arrived(ho.at[pl.ds(0, T - 1)], ho_ss.at[0], ho_rs.at[0])
    span = (T - 2) * VALUE
    early_head = jnp.where(below, 0, 2)
    late_first = jnp.where(below, T - 2, 0)

    def heads_of(first, n):
        return jnp.concatenate(
            [
                jnp.concatenate(
                    [
                        ho[first + h, pl.ds(pl.multiple_of(which * rows, rows), rows), :]
                        for h in range(n)
                    ],
                    axis=1,
                )
                for which in (1 - y, y)
            ],
            axis=0,
        )

    blocks = T // 2
    heads = heads_of(early_head, T - 2)
    early_rows = pl.ds(pl.multiple_of(early_head * VALUE, 2 * VALUE), span)
    for j in range(blocks):
        acc[:, j * width : (j + 1) * width] = jnp.dot(
            heads, wo[early_rows, j * width : (j + 1) * width], preferred_element_type=f32
        )
    when(inner, lambda: wo_relay(2))
    wo_relay(3)
    other_rows = pl.ds(0, (T - 1) * VALUE)
    arrived(wo.at[pl.ds(0, 2 * VALUE), pl.ds(0, 2 * strip)], wo_tss.at[0], wo_trs.at[1])
    heads = heads_of(late_first, 2)
    late_rows = pl.ds(pl.multiple_of(late_first * VALUE, 2 * VALUE), 2 * VALUE)
    near = []
    per_piece = blocks // FAR_PIECES
    for j in range(blocks):
        gated = terms[pl.ds(y * blocks + j, 1), 4:5, :][0] * (
            acc[:, j * width : (j + 1) * width]
            + jnp.dot(heads, wo[late_rows, j * width : (j + 1) * width], preferred_element_type=f32)
        )
        far_send[:, j * width : (j + 1) * width] = gated[:rows].astype(bf16)
        near.append(gated[rows:])
        if (j + 1) % per_piece == 0:
            n = j // per_piece
            piece = pl.ds(n * per_piece * width, per_piece * width)
            send(
                None, far_send.at[:, piece], far_recv.at[:, piece], far_ss.at[n], far_rs.at[n], i, mate
            )
    for j in range(blocks):
        cols = pl.ds(pl.multiple_of(y * half + j * width, width), width)
        out_ref[:, cols] = (lat[own_rows, cols].astype(f32) + near[j]).astype(bf16)
    sent_all(wo.at[other_rows, pl.ds(0, strip)], wo_xss.at[0])
    sent_all(wo.at[other_rows, pl.ds(0, 2 * strip)], wo_tss.at[0])
    sent_all(ho.at[pl.ds(0, T - 1)], ho_ss.at[0])
    for n in range(FAR_PIECES):
        piece = pl.ds(n * per_piece * width, per_piece * width)
        arrived(far_recv.at[:, piece], far_ss.at[n], far_rs.at[n])
        for j in range(n * per_piece, (n + 1) * per_piece):
            cols = pl.ds(pl.multiple_of((1 - y) * half + j * width, width), width)
            out_ref[:, cols] = (
                lat[own_rows, cols].astype(f32)
                + far_recv[:, j * width : (j + 1) * width].astype(f32)
            ).astype(bf16)

    drain()


def fused_shards(S, T, *args):
    (latents, context, condition, context_condition, norm_gain, shift_weight, scale_weight,
     gate_weight, query_weight, key_weight, value_weight, subtract_share, head_gain,
     output_weight) = args
    rows, D = latents.shape
    crows = context.shape[0]
    count = rows * T
    Z = T // 2
    bf16, f32 = jnp.bfloat16, jnp.float32
    vmem = pl.BlockSpec(memory_space=pltpu.VMEM)
    hbm = pl.BlockSpec(memory_space=pltpu.HBM)
    dma = pltpu.SemaphoreType.DMA
    return pl.pallas_call(
        functools.partial(fused_kernel, S=S, T=T),
        out_shape=jax.ShapeDtypeStruct((rows, D), bf16),
        in_specs=[hbm] * 14,
        out_specs=vmem,
        scratch_shapes=[
            pltpu.VMEM((crows, D), bf16),
            pltpu.VMEM((1, condition.shape[0]), f32),
            pltpu.VMEM((1, condition.shape[0]), f32),
            pltpu.VMEM((1, D), f32),
            pltpu.VMEM((1, 1), f32),
            pltpu.VMEM((1, VALUE), f32),
            pltpu.VMEM((count, D), bf16),
            pltpu.VMEM((count // 2, D), bf16),
            pltpu.VMEM((crows, D), bf16),
            pltpu.VMEM((D, 3 * VALUE), bf16),
            pltpu.VMEM((T * VALUE, D // 2), bf16),
            pltpu.VMEM((VALUE, D // (2 * S)), bf16),
            pltpu.VMEM((S, 8, D // T), f32),
            pltpu.VMEM((T, 8, D // T), f32),
            pltpu.VMEM((2, count, VALUE), f32),
            pltpu.VMEM((2 * count, VALUE), bf16),
            pltpu.VMEM((S, count + crows, 2 * VALUE), bf16),
            pltpu.VMEM((count, VALUE), bf16),
            pltpu.VMEM((T, 2 * rows, VALUE), bf16),
            pltpu.VMEM(shift_weight.shape, bf16),
            pltpu.VMEM(shift_weight.shape, bf16),
            pltpu.VMEM(shift_weight.shape, bf16),
            pltpu.VMEM((rows, D // 2), bf16),
            pltpu.VMEM((rows, D // 2), bf16),
            pltpu.VMEM((2 * rows, D // 2), f32),
            dma((16,)), dma((CHUNKS, 4)), dma((CHUNKS, Z + 1)), dma((CHUNKS,)), dma((1,)), dma((2,)),
            dma((1,)), dma((1,)), dma((1,)), dma((1,)), pltpu.SemaphoreType.REGULAR((3,)),
            dma((2, 3)), dma((2, S)), dma((3,)), dma((S,)),
            dma((1,)), dma((1,)), dma((1,)), dma((1,)), dma((T,)), dma((1,)), dma((T,)), dma((1,)), dma((2,)),
            dma((FAR_PIECES,)), dma((FAR_PIECES,)),
        ],
        compiler_params=pltpu.CompilerParams(
            collective_id=0, has_side_effects=True, vmem_limit_bytes=VMEM_LIMIT
        ),
    )(latents, context, condition[None, :], context_condition[None, :], norm_gain[None, :],
      shift_weight, scale_weight, gate_weight, query_weight, key_weight, value_weight,
      subtract_share[None, :], head_gain[None, :], output_weight)


def fits(S, T, shapes):
    rows = shapes[0][0] // (S * T)
    crows = shapes[1][0] // S
    D = shapes[0][1]
    heads = shapes[8][1] // VALUE
    return (
        S == 4 and T == 8 and heads == T and rows % 32 == 0
        and crows % 16 == 0 and D % (128 * T) == 0 and D % (128 * CHUNKS) == 0
        and rows * T * D * 8 + T * VALUE * D * 2 < 24 * 1024 * 1024
    )


def solution(mesh):
    in_specs = (
        P(("sp", "tp"), None),
        P("sp", None),
        P("sp"),
        P("sp"),
        P(),
        P("sp", "tp"),
        P("sp", "tp"),
        P("sp", "tp"),
        P(None, "tp"),
        P(None, "tp"),
        P(None, "tp"),
        P("tp"),
        P(),
        P("tp", None),
    )
    out_specs = P(("sp", "tp"), None)
    S, T = mesh.shape["sp"], mesh.shape["tp"]

    def whole(*args):
        if fits(S, T, [a.shape for a in args]):
            body = functools.partial(fused_shards, S, T)
        else:
            body = shards
        return jax.shard_map(
            body, mesh=mesh, in_specs=in_specs, out_specs=out_specs, check_vma=False
        )(*args)

    return whole
```

```python
import functools
import math

import jax
import jax.numpy as jnp
from jax import lax
from jax.experimental import pallas as pl
from jax.experimental.pallas import tpu as pltpu
from jax.sharding import PartitionSpec as P

HEAD = 64
VALUE = 128
GRID_W = 64


norm_eps = 1e-06
head_eps = 1e-05
rope_theta = 10000.0
head_scale = 0.8


def rotary_tables(positions):
    quarter = HEAD // 4
    inverse = rope_theta ** (-2.0 * jnp.arange(quarter, dtype=jnp.float32) / (HEAD // 2))
    row_angle = (positions // GRID_W).astype(jnp.float32)[:, None] * inverse[None, :]
    column_angle = (positions % GRID_W).astype(jnp.float32)[:, None] * inverse[None, :]
    angles = jnp.concatenate([row_angle, row_angle, column_angle, column_angle], axis=-1)
    return (jnp.cos(angles), jnp.sin(angles))


def rotate(vectors, cosine, sine_table):
    quarter = HEAD // 4
    pieces = vectors.reshape(vectors.shape[:-1] + (2, 2, quarter))
    turned = jnp.concatenate([-pieces[..., 1:, :], pieces[..., :1, :]], axis=-2).reshape(
        vectors.shape
    )
    return vectors * cosine[:, None, :] + turned * sine_table[:, None, :]


def modulate(token_rows, gain_row, shift_row, scale_row):
    widened = token_rows.astype(jnp.float32)
    normed = widened * lax.rsqrt(jnp.mean(widened * widened, axis=-1, keepdims=True) + norm_eps)
    return (normed * gain_row * (1.0 + scale_row) + shift_row).astype(jnp.bfloat16)


def shards(
    latents,
    context,
    condition,
    context_condition,
    norm_gain,
    shift_weight,
    scale_weight,
    gate_weight,
    query_weight,
    key_weight,
    value_weight,
    subtract_share,
    head_gain,
    output_weight,
):
    activated = jax.nn.silu(jnp.stack([condition, context_condition])).astype(jnp.bfloat16)
    partial_terms = jnp.stack(
        [
            jnp.dot(activated, matrix, preferred_element_type=jnp.float32)
            for matrix in (shift_weight, scale_weight, gate_weight)
        ]
    )
    summed = lax.psum(partial_terms, "sp")
    full_terms = lax.all_gather(summed, "tp", axis=2, tiled=True)
    shift_terms, scale_terms, gate_terms = (full_terms[0], full_terms[1], full_terms[2])
    pair_weight = jnp.concatenate([key_weight, value_weight], axis=1)
    joined = jnp.concatenate([query_weight, pair_weight], axis=1)
    projected = jnp.dot(
        modulate(
            lax.all_gather(latents, "tp", axis=0, tiled=True),
            norm_gain,
            shift_terms[0],
            scale_terms[0],
        ),
        joined,
        preferred_element_type=jnp.float32,
    )
    local_count = projected.shape[0]
    positions = lax.axis_index("sp") * local_count + jnp.arange(local_count, dtype=jnp.int32)
    cosine, sine_table = rotary_tables(positions)
    queries = rotate(projected[:, :VALUE].reshape(local_count, 2, HEAD), cosine, sine_table)
    queries = queries.reshape(local_count, VALUE).astype(jnp.bfloat16)
    latent_keys = rotate(
        projected[:, VALUE : 2 * VALUE].reshape(local_count, 2, HEAD), cosine, sine_table
    )
    latent_keys = latent_keys.reshape(local_count, VALUE).astype(jnp.bfloat16)
    latent_pairs = jnp.concatenate(
        [latent_keys, projected[:, 2 * VALUE :].astype(jnp.bfloat16)], axis=1
    )
    context_mod = modulate(context, norm_gain, shift_terms[1], scale_terms[1])
    context_pairs = jnp.dot(context_mod, pair_weight, preferred_element_type=jnp.float32).astype(
        jnp.bfloat16
    )
    sent_pairs = jnp.concatenate([latent_pairs, context_pairs], axis=0)
    arrived = lax.all_gather(sent_pairs, "sp", axis=0, tiled=True)
    updated_carry = []
    for which_map in range(2):
        offset = which_map * HEAD
        scores = jnp.einsum(
            "qd,kd->qk",
            queries[:, offset : offset + HEAD],
            arrived[:, offset : offset + HEAD],
            preferred_element_type=jnp.float32,
        ) * HEAD ** (-0.5)
        powers = jnp.exp(scores)
        updated_carry.append(
            jnp.dot(
                powers.astype(jnp.bfloat16), arrived[:, VALUE:], preferred_element_type=jnp.float32
            )
        )
        updated_carry.append(jnp.sum(powers, axis=1, keepdims=True))
    first_sum, first_total, second_sum, second_total = tuple(updated_carry)
    share_value = subtract_share[0]
    difference = first_sum / first_total - share_value * (second_sum / second_total)
    normed = difference * lax.rsqrt(
        jnp.mean(difference * difference, axis=1, keepdims=True) + head_eps
    )
    head_output = (normed * head_gain * head_scale).astype(jnp.bfloat16)
    branch = lax.psum_scatter(
        jnp.dot(head_output, output_weight, preferred_element_type=jnp.float32),
        "tp",
        scatter_dimension=0,
        tiled=True,
    )
    return (latents.astype(jnp.float32) + gate_terms[0] * branch).astype(jnp.bfloat16)


MESH = pl.DeviceIdType.MESH
CHUNKS = 4
FAR_PIECES = 4
VMEM_LIMIT = 55000 * 1024


def fused_kernel(
    lat_hbm, ctx_hbm, cond_hbm, ccond_hbm, gain_hbm, shift_hbm, scale_hbm, gate_hbm,
    wq_hbm, wk_hbm, wv_hbm, share_hbm, hgain_hbm, wo_hbm, out_ref,
    ctx_ref, cond_ref, ccond_ref, gain_ref, share_ref, hgain_ref, lat, mod, cmod, wqkv, wo, wo_own,
    part, terms, tables, queries, kv, ho_send, ho, shift_ref, scale_ref, gate_ref, far_send, far_recv, acc,
    load_sem, lat_ss, lat_rs, lat_xrs, lat_yss, lat_yrs, part_ss, part_rs, term_ss, term_rs, chain_sem,
    kv_ss, kv_rs, ckv_ss, ckv_rs, ho_ss, ho_rs, wo_mss, wo_ss, wo_rs, wo_xss, wo_xrs, wo_tss, wo_trs,
    far_ss, far_rs,
    *, S, T,
):
    f32, bf16 = jnp.float32, jnp.bfloat16
    count, D = lat.shape
    rows = count // T
    crows = ctx_ref.shape[0]
    width = D // T
    half = D // 2
    strip = half // S
    Z = T // 2
    i = lax.axis_index("sp")
    t = lax.axis_index("tp")
    z = lax.div(t, 2)
    y = lax.rem(t, 2)
    mate = t + 1 - 2 * y
    twin = i + 1 - 2 * lax.rem(i, 2)
    across = lax.rem(i + 2, S)
    twin_across = lax.rem(twin + 2, S)
    inner = jnp.logical_and(z > 0, z < Z - 1)
    outer = jnp.logical_or(z == 0, z == Z - 1)
    pending = []

    def when(cond, action):
        if cond is None:
            action()
        else:
            pl.when(cond)(action)

    def copy(src, dst, ss, rs, sp, tp):
        return pltpu.make_async_remote_copy(
            src_ref=src, dst_ref=dst, send_sem=ss, recv_sem=rs,
            device_id={"sp": sp, "tp": tp}, device_id_type=MESH,
        )

    def send(cond, src, dst, ss, rs, sp, tp, tracked=True):
        made = copy(src, dst, ss, rs, sp, tp)

        def go():
            made.start()

        when(cond, go)
        if tracked:
            pending.append((cond, made))

    def drain():
        for cond, made in pending:
            def finish(made=made):
                made.wait_send()

            when(cond, finish)
        pending.clear()

    def sent_all(view, ss):
        copy(view, view, ss, ss, twin, t).wait_send()

    def arrived(dst, ss, rs):
        copy(dst, dst, ss, rs, twin, t).wait_recv()

    def load(k, src, dst):
        return pltpu.make_async_copy(src, dst, load_sem.at[k])

    def half_cols(which):
        return pl.ds(pl.multiple_of(which * half, half), half)

    def strip_cols(which, share):
        return pl.ds(pl.multiple_of(which * half + share * strip, strip), strip)

    own_rows = pl.ds(pl.multiple_of(t * rows, rows), rows)
    own_load = load(0, lat_hbm, lat.at[own_rows, :])
    cond_loads = [load(1, cond_hbm, cond_ref), load(2, ccond_hbm, ccond_ref)]
    term_loads = [
        load(3, shift_hbm, shift_ref), load(4, scale_hbm, scale_ref), load(5, gate_hbm, gate_ref)
    ]
    qkv_loads = [
        load(6, wq_hbm, wqkv.at[:, pl.ds(0, VALUE)]),
        load(7, wk_hbm, wqkv.at[:, pl.ds(VALUE, VALUE)]),
        load(8, wv_hbm, wqkv.at[:, pl.ds(2 * VALUE, VALUE)]),
        load(9, ctx_hbm, ctx_ref),
        load(10, gain_hbm, gain_ref),
        load(11, share_hbm, share_ref),
        load(12, hgain_hbm, hgain_ref),
    ]
    wo_strip = load(13, wo_hbm.at[:, strip_cols(1 - y, i)], wo_own)
    wo_half = load(15, wo_hbm.at[:, half_cols(y)], wo.at[pl.ds(t * VALUE, VALUE), :])

    barrier = pltpu.get_barrier_semaphore()

    def greet(cond, sp, tp):
        def go():
            pl.semaphore_signal(
                barrier, inc=1, device_id={"sp": sp, "tp": tp}, device_id_type=MESH
            )

        when(cond, go)

    greet(z > 0, i, t - 2)
    greet(z < Z - 1, i, t + 2)
    greet(None, i, mate)
    for peer in (across, twin_across, twin):
        greet(None, peer, t)
    for made in [own_load] + cond_loads + term_loads + [wo_strip, wo_half] + qkv_loads:
        made.start()
    pl.semaphore_wait(
        barrier, 4 + (z > 0).astype(jnp.int32) + (z < Z - 1).astype(jnp.int32)
    )
    def chain(cond, which, tp):
        def go():
            pl.semaphore_signal(
                chain_sem.at[which], inc=1, device_id={"sp": i, "tp": tp}, device_id_type=MESH
            )

        when(cond, go)

    def chained(cond, which):
        def go():
            pl.semaphore_wait(chain_sem.at[which], 1)

        when(cond, go)

    below = z < Z - 1 - z
    inward = jnp.where(below, t + 4, t - 4)
    midward = jnp.where(below, t + 2, t - 2)
    outward = jnp.where(below, t - 2, t + 2)
    chain(inner, 0, outward)
    chain(outer, 1, midward)
    own_load.wait()

    step = D // CHUNKS

    def lat_piece(block, c):
        return lat.at[pl.ds(pl.multiple_of(block * rows, rows), rows), pl.ds(c * step, step)]

    def wo_piece(head, share):
        return wo.at[
            pl.ds(pl.multiple_of(head * VALUE, VALUE), VALUE),
            pl.ds(pl.multiple_of(share * strip, strip), strip),
        ]

    upper = range(CHUNKS // 2, CHUNKS)
    for c in range(CHUNKS):
        own = lat_piece(t, c)
        send(z < Z - 1, own, own, lat_ss.at[c, 0], lat_rs.at[c, z], i, t + 2)
        send(z > 0, own, own, lat_ss.at[c, 1], lat_rs.at[c, z], i, t - 2)
        rs = lat_rs.at[c, Z] if c in upper else lat_yrs.at[0]
        send(None, own, own, lat_yss.at[0], rs, i, mate, False)

    wo_strip.wait()
    send(None, wo_own, wo_piece(t, i), wo_mss.at[0], wo_rs.at[t], i, mate, False)

    def lat_far():
        for c in range(CHUNKS):
            own = lat_piece(t, c)
            send(outer, own, own, lat_ss.at[c, 2], lat_rs.at[c, z], i, inward)

    opposite = 2 * (Z - 1 - z) + y

    def lat_cross():
        for c in upper:
            piece = lat_piece(mate, c)
            arrived(piece, lat_yss.at[0], lat_rs.at[c, Z])
            send(outer, piece, piece, lat_ss.at[c, 3], lat_xrs.at[c], i, opposite)

    def lat_stage(d, chunks=range(CHUNKS)):
        for c in chunks:
            for sign in (-1, 1):
                block = t + 2 * d * sign
                here = z - d >= 0 if sign < 0 else z + d < Z
                piece = lat_piece(block, c)
                layer = z + d * sign
                rs = lat_rs.at[c, layer]

                def come(piece=piece, rs=rs):
                    arrived(piece, lat_yss.at[0], rs)

                when(here, come)
                if d < Z - 1:
                    onward = jnp.logical_and(here, jnp.logical_and(inner, below == (sign > 0)))
                    send(onward, piece, piece, lat_ss.at[c, 1 + d], rs, i, outward)
                if d < Z - 1 or c not in upper:
                    batch = jnp.where((2 * layer < Z) == below, 0, 1)
                    send(here, piece, piece, lat_yss.at[0], lat_yrs.at[batch], i, mate, False)

    def lat_last():
        def come():
            for c in upper:
                arrived(lat_piece(opposite + mate - t, c), lat_yss.at[0], lat_xrs.at[c])

        when(outer, come)

    def wo_launch(cond, head, tp):
        piece = wo_piece(head, i)
        send(cond, piece, piece, wo_ss.at[0], wo_rs.at[head], i, tp, False)

    def wo_heads(d, sign):
        layer = 2 * (z + d * sign)
        return (layer + y, layer + 1 - y)

    def late_head(head):
        layer = lax.div(head, 2)
        return jnp.where(layer == jnp.where(below, Z - 1, 0), 1, 0)

    def wo_take(cond, head, onward=None):
        def go():
            piece = wo_piece(head, i)
            arrived(piece, wo_ss.at[0], wo_rs.at[head])

        when(cond, go)
        if onward is not None:
            wo_launch(onward, head, outward)

    def wo_share(cond, head):
        def go():
            piece = wo_piece(head, i)
            copy(piece, piece, wo_xss.at[0], wo_xrs.at[head], across, t).start()
            copy(piece, piece, wo_tss.at[0], wo_trs.at[late_head(head)], twin, t).start()

        when(cond, go)

    def wo_stage(d, where, middle=None, take=True, share=True):
        for sign in (-1, 1):
            here = z - d >= 0 if sign < 0 else z + d < Z
            here = jnp.logical_and(here, where)
            if middle is not None:
                here = jnp.logical_and(here, (below == (sign > 0)) == middle)
            onward = None
            if d < Z - 1:
                onward = jnp.logical_and(here, jnp.logical_and(inner, below == (sign > 0)))
            for head in wo_heads(d, sign):
                if take:
                    wo_take(here, head, onward)
                if share:
                    wo_share(here, head)

    def wo_relay(d, where=None):
        todo = [(None, mate)] if d == 0 else [
            (z - d >= 0 if sign < 0 else z + d < Z, head)
            for sign in (-1, 1) for head in wo_heads(d, sign)
        ]
        for cond, head in todo:
            def go(head=head):
                piece = wo_piece(head, across)
                arrived(piece, wo_ss.at[0], wo_xrs.at[head])
                copy(piece, piece, wo_tss.at[0], wo_trs.at[late_head(head)], twin, t).start()

            when(cond, go)

    def silu(v):
        return v / (1.0 + jnp.exp(-v))

    for made in cond_loads:
        made.wait()
    depth = cond_ref.shape[1]
    line = lax.broadcasted_iota(jnp.int32, (8, depth), 0)
    act0 = jnp.broadcast_to(silu(cond_ref[...]), (8, depth))
    act1 = jnp.broadcast_to(silu(ccond_ref[...]), (8, depth))

    def two_lines(first, matrix_ref, with_second):
        left = jnp.where(line == first, act0, 0.0)
        if with_second:
            left = jnp.where(line == first + 1, act1, left)
        return jnp.dot(left.astype(bf16), matrix_ref[...], preferred_element_type=f32)

    for made in term_loads:
        made.wait()
    part[pl.ds(i, 1)] = (
        two_lines(0, shift_ref, True) + two_lines(2, scale_ref, True) + two_lines(4, gate_ref, False)
    )[None]
    for k in range(1, S):
        send(None, part.at[i], part.at[i], part_ss.at[0], part_rs.at[0], lax.rem(i + k, S), t, False)

    lane = lax.broadcasted_iota(jnp.int32, (count, VALUE), 1)
    place = i * count + lax.broadcasted_iota(jnp.int32, (count, VALUE), 0)
    spot = lax.rem(lane, HEAD)
    quarter = HEAD // 4
    power = lax.rem(spot, quarter).astype(f32) * (-2.0 / (HEAD // 2))
    inverse = jnp.exp(power * math.log(rope_theta))
    along = jnp.where(spot < HEAD // 2, lax.div(place, GRID_W), lax.rem(place, GRID_W))
    angle = along.astype(f32) * inverse
    even = lax.rem(lax.div(spot, quarter), 2) == 0
    tables[0] = jnp.cos(angle)
    tables[1] = jnp.sin(angle)

    chained(outer, 0)
    lat_far()
    chained(inner, 1)
    chain(inner, 2, midward)
    chained(inner, 2)
    chain(inner, 2, outward)
    lat_stage(1, range(CHUNKS // 2))
    chained(outer, 2)

    arrived(part.at[pl.ds(0, S - 1)], part_ss.at[0], part_rs.at[0])
    total = part[0]
    for k in range(1, S):
        total = total + part[k]
    terms[pl.ds(t, 1)] = total[None]
    for k in range(1, T):
        send(
            None, terms.at[t], terms.at[t], term_ss.at[0], term_rs.at[0], i, lax.rem(t + k, T), False
        )

    lat_stage(1, range(CHUNKS // 2, CHUNKS))
    lat_cross()
    wo_half.wait()
    wo_take(None, mate)
    wo_share(None, mate)
    for head in (t, mate):
        wo_launch(None, head, midward)
    lat_stage(2)
    for head in (t, mate):
        wo_launch(outer, head, inward)
    wo_launch(inner, t, outward)
    wo_launch(inner, mate, outward)
    lat_stage(3, range(CHUNKS // 2))

    def modulate_into(dst, src, first, n, which):
        wide = src[...].astype(f32)
        factor = lax.rsqrt(jnp.mean(wide * wide, axis=-1, keepdims=True) + norm_eps)
        for j in range(T):
            cols = slice(j * width, (j + 1) * width)
            mult = gain_ref[:, cols] * (1.0 + terms[j, 2 + which : 3 + which, :])
            shifted = wide[:, cols] * factor * mult + terms[j, which : which + 1, :]
            dst[pl.ds(first, n), cols] = shifted.astype(bf16)

    def ckv_piece(s):
        return kv.at[s, pl.ds(count, crows), :]

    part_rows = count // 2
    batch_first = [
        pl.multiple_of(jnp.where(below == (b == 0), 0, part_rows), part_rows) for b in range(2)
    ]

    def kv_piece(s, b):
        return kv.at[s, pl.ds(batch_first[b], part_rows), :]

    first_half = lax.broadcasted_iota(jnp.int32, (part_rows, VALUE), 1) < HEAD

    def project_batch(b):
        first = batch_first[b]
        which = pl.ds(first, part_rows)
        modulate_into(mod, lat.at[which, :], 0, part_rows, 0)
        projected = jnp.dot(mod[...], wqkv[...], preferred_element_type=f32)

        def rotated(u):
            turned = jnp.where(
                even[:part_rows], -pltpu.roll(u, VALUE - quarter, 1), pltpu.roll(u, quarter, 1)
            )
            return u * tables[0, which, :] + turned * tables[1, which, :]

        kv[pl.ds(i, 1), which, pl.ds(0, VALUE)] = (
            rotated(projected[:, VALUE : 2 * VALUE]).astype(bf16)[None]
        )
        kv[pl.ds(i, 1), which, pl.ds(VALUE, VALUE)] = projected[:, 2 * VALUE :].astype(bf16)[None]
        own = kv_piece(i, b)
        send(None, own, own, kv_ss.at[b, 0], kv_rs.at[b, i], across, t)
        send(None, own, own, kv_ss.at[b, 1], kv_rs.at[b, i], twin, t)
        query = rotated(projected[:, :VALUE]).astype(bf16) * jnp.asarray(HEAD ** (-0.5), bf16)
        zero = jnp.zeros_like(query)
        queries[which, :] = jnp.where(first_half, query, zero)
        queries[pl.ds(pl.multiple_of(count + first, part_rows), part_rows), :] = jnp.where(
            first_half, zero, query
        )

    def kv_relay(b):
        piece = kv_piece(across, b)
        arrived(piece, kv_ss.at[b, 2], kv_rs.at[b, across])
        send(None, piece, piece, kv_ss.at[b, 2], kv_rs.at[b, across], twin, t)

    for made in qkv_loads:
        made.wait()
    arrived(terms.at[pl.ds(0, T - 1)], term_ss.at[0], term_rs.at[0])
    modulate_into(cmod, ctx_ref, 0, crows, 1)
    kv[pl.ds(i, 1), pl.ds(count, crows), :] = jnp.dot(
        cmod[...], wqkv[:, VALUE:], preferred_element_type=f32
    ).astype(bf16)[None]
    send(None, ckv_piece(i), ckv_piece(i), ckv_ss.at[0], ckv_rs.at[i], across, t)
    send(None, ckv_piece(i), ckv_piece(i), ckv_ss.at[1], ckv_rs.at[i], twin, t)

    def over_wait(n, ss, rs):
        view = lat.at[pl.ds(0, n), :]
        if rs is None:
            sent_all(view, ss)
        else:
            arrived(view, ss, rs)

    over_wait(3 * rows // 2, lat_yss.at[0], lat_yrs.at[0])
    project_batch(0)
    lat_stage(3, upper)
    lat_last()
    wo_stage(1, inner, True, share=False)
    when(outer, lambda: over_wait(3 * rows // 2, lat_yss.at[0], lat_yrs.at[1]))
    when(inner, lambda: over_wait(2 * rows, lat_yss.at[0], lat_yrs.at[1]))
    project_batch(1)
    wo_stage(1, inner, True, take=False)
    wo_stage(2, inner)
    wo_stage(1, outer)
    arrived(ckv_piece(across), ckv_ss.at[2], ckv_rs.at[across])
    send(None, ckv_piece(across), ckv_piece(across), ckv_ss.at[2], ckv_rs.at[across], twin, t)
    kv_relay(0)

    def attend(rows_kv):
        scores = lax.dot_general(
            queries[...], rows_kv[:, :VALUE], (((1,), (1,)), ((), ())), preferred_element_type=f32
        )
        ones = jnp.ones((rows_kv.shape[0], VALUE), bf16)
        return jnp.dot(
            jnp.exp(scores).astype(bf16),
            jnp.concatenate([rows_kv[:, VALUE:], ones], axis=1),
            preferred_element_type=f32,
        )

    def attend_first(s):
        return attend(jnp.concatenate([kv_piece(s, 0)[...], ckv_piece(s)[...]], axis=0))

    sums = attend(kv[i])
    wo_relay(0)
    arrived(kv_piece(twin, 0), kv_ss.at[0, 2], kv_rs.at[0, twin])
    arrived(ckv_piece(twin), ckv_ss.at[2], ckv_rs.at[twin])
    sums = sums + attend_first(twin)
    sums = sums + attend_first(across)
    arrived(kv_piece(twin_across, 0), kv_ss.at[0, 2], kv_rs.at[0, twin_across])
    arrived(ckv_piece(twin_across), ckv_ss.at[2], ckv_rs.at[twin_across])
    sums = sums + attend_first(twin_across)
    wo_stage(1, inner, False)
    arrived(kv_piece(twin, 1), kv_ss.at[1, 2], kv_rs.at[1, twin])
    sums = sums + attend(kv_piece(twin, 1)[...])
    kv_relay(1)
    wo_stage(2, outer)
    sums = sums + attend(kv_piece(across, 1)[...])
    arrived(kv_piece(twin_across, 1), kv_ss.at[1, 2], kv_rs.at[1, twin_across])
    sums = sums + attend(kv_piece(twin_across, 1)[...])
    ratio = sums[:, :VALUE] / sums[:, VALUE:]
    difference = ratio[:count] - share_ref[...] * ratio[count:]
    normed = difference * lax.rsqrt(
        jnp.mean(difference * difference, axis=1, keepdims=True) + head_eps
    )
    ho_send[...] = (normed * hgain_ref[...] * head_scale).astype(bf16)

    def pair_rows(layer):
        return ho_send.at[pl.ds(pl.multiple_of(layer * 2 * rows, 2 * rows), 2 * rows), :]

    for k in range(1, T):
        peer = lax.rem(t + k, T)
        send(None, pair_rows(lax.div(peer, 2)), ho.at[t], ho_ss.at[0], ho_rs.at[0], i, peer, False)
    ho[pl.ds(t, 1)] = pair_rows(z)[...][None]

    wo_stage(3, outer)
    wo_relay(1)
    for where in (outer, inner):
        def second(where=where):
            if where is outer:
                wo_relay(2)

        when(where, second)
    drain()
    when(outer, lambda: over_wait(7 * rows // 2, lat_yss.at[0], None))
    when(inner, lambda: over_wait(4 * rows, lat_yss.at[0], None))
    sent_all(part.at[pl.ds(0, S - 1)], part_ss.at[0])
    sent_all(terms.at[pl.ds(0, T - 1)], term_ss.at[0])
    sent_all(wo_own, wo_mss.at[0])

    def wo_sent(heads):
        def go():
            sent_all(wo.at[pl.ds(0, heads * VALUE), pl.ds(0, strip)], wo_ss.at[0])

        return go

    when(outer, wo_sent(4))
    when(inner, wo_sent(8))
    early_heads = T - 3
    arrived(wo.at[pl.ds(0, early_heads * VALUE), pl.ds(0, 2 * strip)], wo_tss.at[0], wo_trs.at[0])
    arrived(ho.at[pl.ds(0, T - 1)], ho_ss.at[0], ho_rs.at[0])
    span = (T - 2) * VALUE
    early_head = jnp.where(below, 0, 2)
    late_first = jnp.where(below, T - 2, 0)

    def heads_of(first, n):
        return jnp.concatenate(
            [
                jnp.concatenate(
                    [
                        ho[first + h, pl.ds(pl.multiple_of(which * rows, rows), rows), :]
                        for h in range(n)
                    ],
                    axis=1,
                )
                for which in (1 - y, y)
            ],
            axis=0,
        )

    blocks = T // 2
    heads = heads_of(early_head, T - 2)
    early_rows = pl.ds(pl.multiple_of(early_head * VALUE, 2 * VALUE), span)
    for j in range(blocks):
        acc[:, j * width : (j + 1) * width] = jnp.dot(
            heads, wo[early_rows, j * width : (j + 1) * width], preferred_element_type=f32
        )
    when(inner, lambda: wo_relay(2))
    wo_relay(3)
    other_rows = pl.ds(0, (T - 1) * VALUE)
    arrived(wo.at[pl.ds(0, 2 * VALUE), pl.ds(0, 2 * strip)], wo_tss.at[0], wo_trs.at[1])
    heads = heads_of(late_first, 2)
    late_rows = pl.ds(pl.multiple_of(late_first * VALUE, 2 * VALUE), 2 * VALUE)
    near = []
    per_piece = blocks // FAR_PIECES
    for j in range(blocks):
        gated = terms[pl.ds(y * blocks + j, 1), 4:5, :][0] * (
            acc[:, j * width : (j + 1) * width]
            + jnp.dot(heads, wo[late_rows, j * width : (j + 1) * width], preferred_element_type=f32)
        )
        far_send[:, j * width : (j + 1) * width] = gated[:rows].astype(bf16)
        near.append(gated[rows:])
        if (j + 1) % per_piece == 0:
            n = j // per_piece
            piece = pl.ds(n * per_piece * width, per_piece * width)
            send(
                None, far_send.at[:, piece], far_recv.at[:, piece], far_ss.at[n], far_rs.at[n], i, mate
            )
    for j in range(blocks):
        cols = pl.ds(pl.multiple_of(y * half + j * width, width), width)
        out_ref[:, cols] = (lat[own_rows, cols].astype(f32) + near[j]).astype(bf16)
    sent_all(wo.at[other_rows, pl.ds(0, strip)], wo_xss.at[0])
    sent_all(wo.at[other_rows, pl.ds(0, 2 * strip)], wo_tss.at[0])
    sent_all(ho.at[pl.ds(0, T - 1)], ho_ss.at[0])
    for n in range(FAR_PIECES):
        piece = pl.ds(n * per_piece * width, per_piece * width)
        arrived(far_recv.at[:, piece], far_ss.at[n], far_rs.at[n])
        for j in range(n * per_piece, (n + 1) * per_piece):
            cols = pl.ds(pl.multiple_of((1 - y) * half + j * width, width), width)
            out_ref[:, cols] = (
                lat[own_rows, cols].astype(f32)
                + far_recv[:, j * width : (j + 1) * width].astype(f32)
            ).astype(bf16)

    drain()


def fused_shards(S, T, *args):
    (latents, context, condition, context_condition, norm_gain, shift_weight, scale_weight,
     gate_weight, query_weight, key_weight, value_weight, subtract_share, head_gain,
     output_weight) = args
    rows, D = latents.shape
    crows = context.shape[0]
    count = rows * T
    Z = T // 2
    bf16, f32 = jnp.bfloat16, jnp.float32
    vmem = pl.BlockSpec(memory_space=pltpu.VMEM)
    hbm = pl.BlockSpec(memory_space=pltpu.HBM)
    dma = pltpu.SemaphoreType.DMA
    return pl.pallas_call(
        functools.partial(fused_kernel, S=S, T=T),
        out_shape=jax.ShapeDtypeStruct((rows, D), bf16),
        in_specs=[hbm] * 14,
        out_specs=vmem,
        scratch_shapes=[
            pltpu.VMEM((crows, D), bf16),
            pltpu.VMEM((1, condition.shape[0]), f32),
            pltpu.VMEM((1, condition.shape[0]), f32),
            pltpu.VMEM((1, D), f32),
            pltpu.VMEM((1, 1), f32),
            pltpu.VMEM((1, VALUE), f32),
            pltpu.VMEM((count, D), bf16),
            pltpu.VMEM((count // 2, D), bf16),
            pltpu.VMEM((crows, D), bf16),
            pltpu.VMEM((D, 3 * VALUE), bf16),
            pltpu.VMEM((T * VALUE, D // 2), bf16),
            pltpu.VMEM((VALUE, D // (2 * S)), bf16),
            pltpu.VMEM((S, 8, D // T), f32),
            pltpu.VMEM((T, 8, D // T), f32),
            pltpu.VMEM((2, count, VALUE), f32),
            pltpu.VMEM((2 * count, VALUE), bf16),
            pltpu.VMEM((S, count + crows, 2 * VALUE), bf16),
            pltpu.VMEM((count, VALUE), bf16),
            pltpu.VMEM((T, 2 * rows, VALUE), bf16),
            pltpu.VMEM(shift_weight.shape, bf16),
            pltpu.VMEM(shift_weight.shape, bf16),
            pltpu.VMEM(shift_weight.shape, bf16),
            pltpu.VMEM((rows, D // 2), bf16),
            pltpu.VMEM((rows, D // 2), bf16),
            pltpu.VMEM((2 * rows, D // 2), f32),
            dma((16,)), dma((CHUNKS, 4)), dma((CHUNKS, Z + 1)), dma((CHUNKS,)), dma((1,)), dma((2,)),
            dma((1,)), dma((1,)), dma((1,)), dma((1,)), pltpu.SemaphoreType.REGULAR((3,)),
            dma((2, 3)), dma((2, S)), dma((3,)), dma((S,)),
            dma((1,)), dma((1,)), dma((1,)), dma((1,)), dma((T,)), dma((1,)), dma((T,)), dma((1,)), dma((2,)),
            dma((FAR_PIECES,)), dma((FAR_PIECES,)),
        ],
        compiler_params=pltpu.CompilerParams(
            collective_id=0, has_side_effects=True, vmem_limit_bytes=VMEM_LIMIT
        ),
    )(latents, context, condition[None, :], context_condition[None, :], norm_gain[None, :],
      shift_weight, scale_weight, gate_weight, query_weight, key_weight, value_weight,
      subtract_share[None, :], head_gain[None, :], output_weight)


def fits(S, T, shapes):
    rows = shapes[0][0] // (S * T)
    crows = shapes[1][0] // S
    D = shapes[0][1]
    heads = shapes[8][1] // VALUE
    return (
        S == 4 and T == 8 and heads == T and rows % 32 == 0
        and crows % 16 == 0 and D % (128 * T) == 0 and D % (128 * CHUNKS) == 0
        and rows * T * D * 8 + T * VALUE * D * 2 < 24 * 1024 * 1024
    )


def solution(mesh):
    in_specs = (
        P(("sp", "tp"), None),
        P("sp", None),
        P("sp"),
        P("sp"),
        P(),
        P("sp", "tp"),
        P("sp", "tp"),
        P("sp", "tp"),
        P(None, "tp"),
        P(None, "tp"),
        P(None, "tp"),
        P("tp"),
        P(),
        P("tp", None),
    )
    out_specs = P(("sp", "tp"), None)
    S, T = mesh.shape["sp"], mesh.shape["tp"]

    def whole(*args):
        if fits(S, T, [a.shape for a in args]):
            body = functools.partial(fused_shards, S, T)
        else:
            body = shards
        return jax.shard_map(
            body, mesh=mesh, in_specs=in_specs, out_specs=out_specs, check_vma=False
        )(*args)

    return whole
```

```python
import functools
import math

import jax
import jax.numpy as jnp
from jax import lax
from jax.experimental import pallas as pl
from jax.experimental.pallas import tpu as pltpu
from jax.sharding import PartitionSpec as P

HEAD = 64
VALUE = 128
GRID_W = 64


norm_eps = 1e-06
head_eps = 1e-05
rope_theta = 10000.0
head_scale = 0.8


def rotary_tables(positions):
    quarter = HEAD // 4
    inverse = rope_theta ** (-2.0 * jnp.arange(quarter, dtype=jnp.float32) / (HEAD // 2))
    row_angle = (positions // GRID_W).astype(jnp.float32)[:, None] * inverse[None, :]
    column_angle = (positions % GRID_W).astype(jnp.float32)[:, None] * inverse[None, :]
    angles = jnp.concatenate([row_angle, row_angle, column_angle, column_angle], axis=-1)
    return (jnp.cos(angles), jnp.sin(angles))


def rotate(vectors, cosine, sine_table):
    quarter = HEAD // 4
    pieces = vectors.reshape(vectors.shape[:-1] + (2, 2, quarter))
    turned = jnp.concatenate([-pieces[..., 1:, :], pieces[..., :1, :]], axis=-2).reshape(
        vectors.shape
    )
    return vectors * cosine[:, None, :] + turned * sine_table[:, None, :]


def modulate(token_rows, gain_row, shift_row, scale_row):
    widened = token_rows.astype(jnp.float32)
    normed = widened * lax.rsqrt(jnp.mean(widened * widened, axis=-1, keepdims=True) + norm_eps)
    return (normed * gain_row * (1.0 + scale_row) + shift_row).astype(jnp.bfloat16)


def shards(
    latents,
    context,
    condition,
    context_condition,
    norm_gain,
    shift_weight,
    scale_weight,
    gate_weight,
    query_weight,
    key_weight,
    value_weight,
    subtract_share,
    head_gain,
    output_weight,
):
    activated = jax.nn.silu(jnp.stack([condition, context_condition])).astype(jnp.bfloat16)
    partial_terms = jnp.stack(
        [
            jnp.dot(activated, matrix, preferred_element_type=jnp.float32)
            for matrix in (shift_weight, scale_weight, gate_weight)
        ]
    )
    summed = lax.psum(partial_terms, "sp")
    full_terms = lax.all_gather(summed, "tp", axis=2, tiled=True)
    shift_terms, scale_terms, gate_terms = (full_terms[0], full_terms[1], full_terms[2])
    pair_weight = jnp.concatenate([key_weight, value_weight], axis=1)
    joined = jnp.concatenate([query_weight, pair_weight], axis=1)
    projected = jnp.dot(
        modulate(
            lax.all_gather(latents, "tp", axis=0, tiled=True),
            norm_gain,
            shift_terms[0],
            scale_terms[0],
        ),
        joined,
        preferred_element_type=jnp.float32,
    )
    local_count = projected.shape[0]
    positions = lax.axis_index("sp") * local_count + jnp.arange(local_count, dtype=jnp.int32)
    cosine, sine_table = rotary_tables(positions)
    queries = rotate(projected[:, :VALUE].reshape(local_count, 2, HEAD), cosine, sine_table)
    queries = queries.reshape(local_count, VALUE).astype(jnp.bfloat16)
    latent_keys = rotate(
        projected[:, VALUE : 2 * VALUE].reshape(local_count, 2, HEAD), cosine, sine_table
    )
    latent_keys = latent_keys.reshape(local_count, VALUE).astype(jnp.bfloat16)
    latent_pairs = jnp.concatenate(
        [latent_keys, projected[:, 2 * VALUE :].astype(jnp.bfloat16)], axis=1
    )
    context_mod = modulate(context, norm_gain, shift_terms[1], scale_terms[1])
    context_pairs = jnp.dot(context_mod, pair_weight, preferred_element_type=jnp.float32).astype(
        jnp.bfloat16
    )
    sent_pairs = jnp.concatenate([latent_pairs, context_pairs], axis=0)
    arrived = lax.all_gather(sent_pairs, "sp", axis=0, tiled=True)
    updated_carry = []
    for which_map in range(2):
        offset = which_map * HEAD
        scores = jnp.einsum(
            "qd,kd->qk",
            queries[:, offset : offset + HEAD],
            arrived[:, offset : offset + HEAD],
            preferred_element_type=jnp.float32,
        ) * HEAD ** (-0.5)
        powers = jnp.exp(scores)
        updated_carry.append(
            jnp.dot(
                powers.astype(jnp.bfloat16), arrived[:, VALUE:], preferred_element_type=jnp.float32
            )
        )
        updated_carry.append(jnp.sum(powers, axis=1, keepdims=True))
    first_sum, first_total, second_sum, second_total = tuple(updated_carry)
    share_value = subtract_share[0]
    difference = first_sum / first_total - share_value * (second_sum / second_total)
    normed = difference * lax.rsqrt(
        jnp.mean(difference * difference, axis=1, keepdims=True) + head_eps
    )
    head_output = (normed * head_gain * head_scale).astype(jnp.bfloat16)
    branch = lax.psum_scatter(
        jnp.dot(head_output, output_weight, preferred_element_type=jnp.float32),
        "tp",
        scatter_dimension=0,
        tiled=True,
    )
    return (latents.astype(jnp.float32) + gate_terms[0] * branch).astype(jnp.bfloat16)


MESH = pl.DeviceIdType.MESH
CHUNKS = 4
FAR_PIECES = 4
VMEM_LIMIT = 55000 * 1024


def fused_kernel(
    lat_hbm, ctx_hbm, cond_hbm, ccond_hbm, gain_hbm, shift_hbm, scale_hbm, gate_hbm,
    wq_hbm, wk_hbm, wv_hbm, share_hbm, hgain_hbm, wo_hbm, out_ref,
    ctx_ref, cond_ref, ccond_ref, gain_ref, share_ref, hgain_ref, lat, mod, cmod, wqkv, wo, wo_own,
    part, terms, tables, queries, kv, ho_send, ho, shift_ref, scale_ref, gate_ref, far_send, far_recv, acc, last_heads,
    load_sem, lat_ss, lat_rs, lat_xrs, lat_yss, lat_yrs, part_ss, part_rs, term_ss, term_rs, chain_sem,
    kv_ss, kv_rs, ckv_ss, ckv_rs, ho_ss, ho_rs, wo_mss, wo_ss, wo_rs, wo_xss, wo_xrs, wo_tss, wo_trs,
    far_ss, far_rs,
    *, S, T,
):
    f32, bf16 = jnp.float32, jnp.bfloat16
    count, D = lat.shape
    rows = count // T
    crows = ctx_ref.shape[0]
    width = D // T
    half = D // 2
    strip = half // S
    Z = T // 2
    i = lax.axis_index("sp")
    t = lax.axis_index("tp")
    z = lax.div(t, 2)
    y = lax.rem(t, 2)
    mate = t + 1 - 2 * y
    twin = i + 1 - 2 * lax.rem(i, 2)
    across = lax.rem(i + 2, S)
    twin_across = lax.rem(twin + 2, S)
    inner = jnp.logical_and(z > 0, z < Z - 1)
    outer = jnp.logical_or(z == 0, z == Z - 1)
    pending = []

    def when(cond, action):
        if cond is None:
            action()
        else:
            pl.when(cond)(action)

    def copy(src, dst, ss, rs, sp, tp):
        return pltpu.make_async_remote_copy(
            src_ref=src, dst_ref=dst, send_sem=ss, recv_sem=rs,
            device_id={"sp": sp, "tp": tp}, device_id_type=MESH,
        )

    def send(cond, src, dst, ss, rs, sp, tp, tracked=True):
        made = copy(src, dst, ss, rs, sp, tp)

        def go():
            made.start()

        when(cond, go)
        if tracked:
            pending.append((cond, made))

    def drain():
        for cond, made in pending:
            def finish(made=made):
                made.wait_send()

            when(cond, finish)
        pending.clear()

    def sent_all(view, ss):
        copy(view, view, ss, ss, twin, t).wait_send()

    def arrived(dst, ss, rs):
        copy(dst, dst, ss, rs, twin, t).wait_recv()

    def load(k, src, dst):
        return pltpu.make_async_copy(src, dst, load_sem.at[k])

    def half_cols(which):
        return pl.ds(pl.multiple_of(which * half, half), half)

    def strip_cols(which, share):
        return pl.ds(pl.multiple_of(which * half + share * strip, strip), strip)

    own_rows = pl.ds(pl.multiple_of(t * rows, rows), rows)
    own_load = load(0, lat_hbm, lat.at[own_rows, :])
    cond_loads = [load(1, cond_hbm, cond_ref), load(2, ccond_hbm, ccond_ref)]
    term_loads = [
        load(3, shift_hbm, shift_ref), load(4, scale_hbm, scale_ref), load(5, gate_hbm, gate_ref)
    ]
    qkv_loads = [
        load(6, wq_hbm, wqkv.at[:, pl.ds(0, VALUE)]),
        load(7, wk_hbm, wqkv.at[:, pl.ds(VALUE, VALUE)]),
        load(8, wv_hbm, wqkv.at[:, pl.ds(2 * VALUE, VALUE)]),
        load(9, ctx_hbm, ctx_ref),
        load(10, gain_hbm, gain_ref),
        load(11, share_hbm, share_ref),
        load(12, hgain_hbm, hgain_ref),
    ]
    wo_strip = load(13, wo_hbm.at[:, strip_cols(1 - y, i)], wo_own)
    wo_half = load(15, wo_hbm.at[:, half_cols(y)], wo.at[pl.ds(t * VALUE, VALUE), :])

    barrier = pltpu.get_barrier_semaphore()

    def greet(cond, sp, tp):
        def go():
            pl.semaphore_signal(
                barrier, inc=1, device_id={"sp": sp, "tp": tp}, device_id_type=MESH
            )

        when(cond, go)

    greet(z > 0, i, t - 2)
    greet(z < Z - 1, i, t + 2)
    greet(None, i, mate)
    for peer in (across, twin_across, twin):
        greet(None, peer, t)
    for made in [own_load] + cond_loads + term_loads + [wo_strip, wo_half] + qkv_loads:
        made.start()
    pl.semaphore_wait(
        barrier, 4 + (z > 0).astype(jnp.int32) + (z < Z - 1).astype(jnp.int32)
    )
    def chain(cond, which, tp):
        def go():
            pl.semaphore_signal(
                chain_sem.at[which], inc=1, device_id={"sp": i, "tp": tp}, device_id_type=MESH
            )

        when(cond, go)

    def chained(cond, which):
        def go():
            pl.semaphore_wait(chain_sem.at[which], 1)

        when(cond, go)

    below = z < Z - 1 - z
    inward = jnp.where(below, t + 4, t - 4)
    midward = jnp.where(below, t + 2, t - 2)
    outward = jnp.where(below, t - 2, t + 2)
    chain(inner, 0, outward)
    chain(outer, 1, midward)
    own_load.wait()

    step = D // CHUNKS

    def lat_piece(block, c):
        return lat.at[pl.ds(pl.multiple_of(block * rows, rows), rows), pl.ds(c * step, step)]

    def wo_piece(head, share):
        return wo.at[
            pl.ds(pl.multiple_of(head * VALUE, VALUE), VALUE),
            pl.ds(pl.multiple_of(share * strip, strip), strip),
        ]

    upper = range(CHUNKS // 2, CHUNKS)
    for c in range(CHUNKS):
        own = lat_piece(t, c)
        send(z < Z - 1, own, own, lat_ss.at[c, 0], lat_rs.at[c, z], i, t + 2)
        send(z > 0, own, own, lat_ss.at[c, 1], lat_rs.at[c, z], i, t - 2)
        rs = lat_rs.at[c, Z] if c in upper else lat_yrs.at[0]
        send(None, own, own, lat_yss.at[0], rs, i, mate, False)

    wo_strip.wait()
    send(None, wo_own, wo_piece(t, i), wo_mss.at[0], wo_rs.at[t], i, mate, False)

    def lat_far():
        for c in range(CHUNKS):
            own = lat_piece(t, c)
            send(outer, own, own, lat_ss.at[c, 2], lat_rs.at[c, z], i, inward)

    opposite = 2 * (Z - 1 - z) + y

    def lat_cross():
        for c in upper:
            piece = lat_piece(mate, c)
            arrived(piece, lat_yss.at[0], lat_rs.at[c, Z])
            send(outer, piece, piece, lat_ss.at[c, 3], lat_xrs.at[c], i, opposite)

    def lat_stage(d, chunks=range(CHUNKS)):
        for c in chunks:
            for sign in (-1, 1):
                block = t + 2 * d * sign
                here = z - d >= 0 if sign < 0 else z + d < Z
                piece = lat_piece(block, c)
                layer = z + d * sign
                rs = lat_rs.at[c, layer]

                def come(piece=piece, rs=rs):
                    arrived(piece, lat_yss.at[0], rs)

                when(here, come)
                if d < Z - 1:
                    onward = jnp.logical_and(here, jnp.logical_and(inner, below == (sign > 0)))
                    send(onward, piece, piece, lat_ss.at[c, 1 + d], rs, i, outward)
                if d < Z - 1 or c not in upper:
                    batch = jnp.where((2 * layer < Z) == below, 0, 1)
                    send(here, piece, piece, lat_yss.at[0], lat_yrs.at[batch], i, mate, False)

    def lat_last():
        def come():
            for c in upper:
                arrived(lat_piece(opposite + mate - t, c), lat_yss.at[0], lat_xrs.at[c])

        when(outer, come)

    def wo_launch(cond, head, tp):
        piece = wo_piece(head, i)
        send(cond, piece, piece, wo_ss.at[0], wo_rs.at[head], i, tp, False)

    def wo_heads(d, sign):
        layer = 2 * (z + d * sign)
        return (layer + y, layer + 1 - y)

    def late_head(head):
        layer = lax.div(head, 2)
        return jnp.where(layer == jnp.where(below, Z - 1, 0), 1, 0)

    def wo_take(cond, head, onward=None):
        def go():
            piece = wo_piece(head, i)
            arrived(piece, wo_ss.at[0], wo_rs.at[head])

        when(cond, go)
        if onward is not None:
            wo_launch(onward, head, outward)

    def wo_share(cond, head):
        def go():
            piece = wo_piece(head, i)
            copy(piece, piece, wo_xss.at[0], wo_xrs.at[head], across, t).start()
            copy(piece, piece, wo_tss.at[0], wo_trs.at[late_head(head)], twin, t).start()

        when(cond, go)

    def wo_stage(d, where, middle=None, take=True, share=True):
        for sign in (-1, 1):
            here = z - d >= 0 if sign < 0 else z + d < Z
            here = jnp.logical_and(here, where)
            if middle is not None:
                here = jnp.logical_and(here, (below == (sign > 0)) == middle)
            onward = None
            if d < Z - 1:
                onward = jnp.logical_and(here, jnp.logical_and(inner, below == (sign > 0)))
            for head in wo_heads(d, sign):
                if take:
                    wo_take(here, head, onward)
                if share:
                    wo_share(here, head)

    def wo_relay(d, where=None):
        todo = [(None, mate)] if d == 0 else [
            (z - d >= 0 if sign < 0 else z + d < Z, head)
            for sign in (-1, 1) for head in wo_heads(d, sign)
        ]
        for cond, head in todo:
            def go(head=head):
                piece = wo_piece(head, across)
                arrived(piece, wo_ss.at[0], wo_xrs.at[head])
                copy(piece, piece, wo_tss.at[0], wo_trs.at[late_head(head)], twin, t).start()

            when(cond, go)

    def silu(v):
        return v / (1.0 + jnp.exp(-v))

    for made in cond_loads:
        made.wait()
    depth = cond_ref.shape[1]
    line = lax.broadcasted_iota(jnp.int32, (8, depth), 0)
    act0 = jnp.broadcast_to(silu(cond_ref[...]), (8, depth))
    act1 = jnp.broadcast_to(silu(ccond_ref[...]), (8, depth))

    def two_lines(first, matrix_ref, with_second):
        left = jnp.where(line == first, act0, 0.0)
        if with_second:
            left = jnp.where(line == first + 1, act1, left)
        return jnp.dot(left.astype(bf16), matrix_ref[...], preferred_element_type=f32)

    for made in term_loads:
        made.wait()
    part[pl.ds(i, 1)] = (
        two_lines(0, shift_ref, True) + two_lines(2, scale_ref, True) + two_lines(4, gate_ref, False)
    )[None]
    for k in range(1, S):
        send(None, part.at[i], part.at[i], part_ss.at[0], part_rs.at[0], lax.rem(i + k, S), t, False)

    lane = lax.broadcasted_iota(jnp.int32, (count, VALUE), 1)
    place = i * count + lax.broadcasted_iota(jnp.int32, (count, VALUE), 0)
    spot = lax.rem(lane, HEAD)
    quarter = HEAD // 4
    power = lax.rem(spot, quarter).astype(f32) * (-2.0 / (HEAD // 2))
    inverse = jnp.exp(power * math.log(rope_theta))
    along = jnp.where(spot < HEAD // 2, lax.div(place, GRID_W), lax.rem(place, GRID_W))
    angle = along.astype(f32) * inverse
    even = lax.rem(lax.div(spot, quarter), 2) == 0
    tables[0] = jnp.cos(angle)
    tables[1] = jnp.sin(angle)

    chained(outer, 0)
    lat_far()
    chained(inner, 1)
    chain(inner, 2, midward)
    chained(inner, 2)
    chain(inner, 2, outward)
    lat_stage(1, range(CHUNKS // 2))
    chained(outer, 2)

    arrived(part.at[pl.ds(0, S - 1)], part_ss.at[0], part_rs.at[0])
    total = part[0]
    for k in range(1, S):
        total = total + part[k]
    terms[pl.ds(t, 1)] = total[None]
    for k in range(1, T):
        send(
            None, terms.at[t], terms.at[t], term_ss.at[0], term_rs.at[0], i, lax.rem(t + k, T), False
        )

    lat_stage(1, range(CHUNKS // 2, CHUNKS))
    lat_cross()
    wo_half.wait()
    wo_take(None, mate)
    wo_share(None, mate)
    for head in (t, mate):
        wo_launch(None, head, midward)
    lat_stage(2)
    for head in (t, mate):
        wo_launch(outer, head, inward)
    wo_launch(inner, t, outward)
    wo_launch(inner, mate, outward)
    lat_stage(3, range(CHUNKS // 2))

    def modulate_into(dst, src, first, n, which):
        wide = src[...].astype(f32)
        factor = lax.rsqrt(jnp.mean(wide * wide, axis=-1, keepdims=True) + norm_eps)
        for j in range(T):
            cols = slice(j * width, (j + 1) * width)
            mult = gain_ref[:, cols] * (1.0 + terms[j, 2 + which : 3 + which, :])
            shifted = wide[:, cols] * factor * mult + terms[j, which : which + 1, :]
            dst[pl.ds(first, n), cols] = shifted.astype(bf16)

    def ckv_piece(s):
        return kv.at[s, pl.ds(count, crows), :]

    part_rows = count // 2
    batch_first = [
        pl.multiple_of(jnp.where(below == (b == 0), 0, part_rows), part_rows) for b in range(2)
    ]

    def kv_piece(s, b):
        return kv.at[s, pl.ds(batch_first[b], part_rows), :]

    first_half = lax.broadcasted_iota(jnp.int32, (part_rows, VALUE), 1) < HEAD

    def project_batch(b):
        first = batch_first[b]
        which = pl.ds(first, part_rows)
        modulate_into(mod, lat.at[which, :], 0, part_rows, 0)
        projected = jnp.dot(mod[...], wqkv[...], preferred_element_type=f32)

        def rotated(u):
            turned = jnp.where(
                even[:part_rows], -pltpu.roll(u, VALUE - quarter, 1), pltpu.roll(u, quarter, 1)
            )
            return u * tables[0, which, :] + turned * tables[1, which, :]

        kv[pl.ds(i, 1), which, pl.ds(0, VALUE)] = (
            rotated(projected[:, VALUE : 2 * VALUE]).astype(bf16)[None]
        )
        kv[pl.ds(i, 1), which, pl.ds(VALUE, VALUE)] = projected[:, 2 * VALUE :].astype(bf16)[None]
        own = kv_piece(i, b)
        send(None, own, own, kv_ss.at[b, 0], kv_rs.at[b, i], across, t)
        send(None, own, own, kv_ss.at[b, 1], kv_rs.at[b, i], twin, t)
        query = rotated(projected[:, :VALUE]).astype(bf16) * jnp.asarray(HEAD ** (-0.5), bf16)
        zero = jnp.zeros_like(query)
        queries[which, :] = jnp.where(first_half, query, zero)
        queries[pl.ds(pl.multiple_of(count + first, part_rows), part_rows), :] = jnp.where(
            first_half, zero, query
        )

    def kv_relay(b):
        piece = kv_piece(across, b)
        arrived(piece, kv_ss.at[b, 2], kv_rs.at[b, across])
        send(None, piece, piece, kv_ss.at[b, 2], kv_rs.at[b, across], twin, t)

    for made in qkv_loads:
        made.wait()
    arrived(terms.at[pl.ds(0, T - 1)], term_ss.at[0], term_rs.at[0])
    modulate_into(cmod, ctx_ref, 0, crows, 1)
    kv[pl.ds(i, 1), pl.ds(count, crows), :] = jnp.dot(
        cmod[...], wqkv[:, VALUE:], preferred_element_type=f32
    ).astype(bf16)[None]
    send(None, ckv_piece(i), ckv_piece(i), ckv_ss.at[0], ckv_rs.at[i], across, t)
    send(None, ckv_piece(i), ckv_piece(i), ckv_ss.at[1], ckv_rs.at[i], twin, t)

    def over_wait(n, ss, rs):
        view = lat.at[pl.ds(0, n), :]
        if rs is None:
            sent_all(view, ss)
        else:
            arrived(view, ss, rs)

    over_wait(3 * rows // 2, lat_yss.at[0], lat_yrs.at[0])
    project_batch(0)
    lat_stage(3, upper)
    lat_last()
    wo_stage(1, inner, True, share=False)
    when(outer, lambda: over_wait(3 * rows // 2, lat_yss.at[0], lat_yrs.at[1]))
    when(inner, lambda: over_wait(2 * rows, lat_yss.at[0], lat_yrs.at[1]))
    project_batch(1)
    wo_stage(1, inner, False)
    wo_stage(1, inner, True, take=False)
    wo_stage(2, inner)
    wo_stage(1, outer)
    arrived(ckv_piece(across), ckv_ss.at[2], ckv_rs.at[across])
    send(None, ckv_piece(across), ckv_piece(across), ckv_ss.at[2], ckv_rs.at[across], twin, t)
    kv_relay(0)

    def attend(rows_kv):
        scores = lax.dot_general(
            queries[...], rows_kv[:, :VALUE], (((1,), (1,)), ((), ())), preferred_element_type=f32
        )
        ones = jnp.ones((rows_kv.shape[0], VALUE), bf16)
        return jnp.dot(
            jnp.exp(scores).astype(bf16),
            jnp.concatenate([rows_kv[:, VALUE:], ones], axis=1),
            preferred_element_type=f32,
        )

    def attend_first(s):
        return attend(jnp.concatenate([kv_piece(s, 0)[...], ckv_piece(s)[...]], axis=0))

    sums = attend(kv[i])
    wo_relay(0)
    arrived(kv_piece(twin, 0), kv_ss.at[0, 2], kv_rs.at[0, twin])
    arrived(ckv_piece(twin), ckv_ss.at[2], ckv_rs.at[twin])
    sums = sums + attend_first(twin)
    sums = sums + attend_first(across)
    arrived(kv_piece(twin_across, 0), kv_ss.at[0, 2], kv_rs.at[0, twin_across])
    arrived(ckv_piece(twin_across), ckv_ss.at[2], ckv_rs.at[twin_across])
    sums = sums + attend_first(twin_across)
    arrived(kv_piece(twin, 1), kv_ss.at[1, 2], kv_rs.at[1, twin])
    sums = sums + attend(kv_piece(twin, 1)[...])
    kv_relay(1)
    wo_stage(2, outer)
    sums = sums + attend(kv_piece(across, 1)[...])
    arrived(kv_piece(twin_across, 1), kv_ss.at[1, 2], kv_rs.at[1, twin_across])
    sums = sums + attend(kv_piece(twin_across, 1)[...])
    ratio = sums[:, :VALUE] / sums[:, VALUE:]
    difference = ratio[:count] - share_ref[...] * ratio[count:]
    normed = difference * lax.rsqrt(
        jnp.mean(difference * difference, axis=1, keepdims=True) + head_eps
    )
    ho_send[...] = (normed * hgain_ref[...] * head_scale).astype(bf16)

    def pair_rows(layer):
        return ho_send.at[pl.ds(pl.multiple_of(layer * 2 * rows, 2 * rows), 2 * rows), :]

    for k in range(1, T):
        peer = lax.rem(t + k, T)
        send(None, pair_rows(lax.div(peer, 2)), ho.at[t], ho_ss.at[0], ho_rs.at[0], i, peer, False)
    ho[pl.ds(t, 1)] = pair_rows(z)[...][None]

    wo_stage(3, outer)
    wo_relay(1)
    for where in (outer, inner):
        def second(where=where):
            if where is outer:
                wo_relay(2)

        when(where, second)
    drain()
    when(outer, lambda: over_wait(7 * rows // 2, lat_yss.at[0], None))
    when(inner, lambda: over_wait(4 * rows, lat_yss.at[0], None))
    sent_all(part.at[pl.ds(0, S - 1)], part_ss.at[0])
    sent_all(terms.at[pl.ds(0, T - 1)], term_ss.at[0])
    sent_all(wo_own, wo_mss.at[0])

    def wo_sent(heads):
        def go():
            sent_all(wo.at[pl.ds(0, heads * VALUE), pl.ds(0, strip)], wo_ss.at[0])

        return go

    when(outer, wo_sent(4))
    when(inner, wo_sent(8))
    early_heads = T - 3
    arrived(wo.at[pl.ds(0, early_heads * VALUE), pl.ds(0, 2 * strip)], wo_tss.at[0], wo_trs.at[0])
    arrived(ho.at[pl.ds(0, T - 1)], ho_ss.at[0], ho_rs.at[0])
    span = (T - 2) * VALUE
    early_head = jnp.where(below, 0, 2)
    late_first = jnp.where(below, T - 2, 0)

    def heads_of(first, n):
        return jnp.concatenate(
            [
                jnp.concatenate(
                    [
                        ho[first + h, pl.ds(pl.multiple_of(which * rows, rows), rows), :]
                        for h in range(n)
                    ],
                    axis=1,
                )
                for which in (1 - y, y)
            ],
            axis=0,
        )

    blocks = T // 2
    heads = heads_of(early_head, T - 2)
    early_rows = pl.ds(pl.multiple_of(early_head * VALUE, 2 * VALUE), span)
    for j in range(blocks):
        acc[:, j * width : (j + 1) * width] = jnp.dot(
            heads, wo[early_rows, j * width : (j + 1) * width], preferred_element_type=f32
        )
    last_heads[...] = heads_of(late_first, 2)
    when(inner, lambda: wo_relay(2))
    wo_relay(3)
    other_rows = pl.ds(0, (T - 1) * VALUE)
    arrived(wo.at[pl.ds(0, 2 * VALUE), pl.ds(0, 2 * strip)], wo_tss.at[0], wo_trs.at[1])
    heads = last_heads[...]
    late_rows = pl.ds(pl.multiple_of(late_first * VALUE, 2 * VALUE), 2 * VALUE)
    near = []
    per_piece = blocks // FAR_PIECES
    for j in range(blocks):
        gated = terms[pl.ds(y * blocks + j, 1), 4:5, :][0] * (
            acc[:, j * width : (j + 1) * width]
            + jnp.dot(heads, wo[late_rows, j * width : (j + 1) * width], preferred_element_type=f32)
        )
        far_send[:, j * width : (j + 1) * width] = gated[:rows].astype(bf16)
        near.append(gated[rows:])
        if (j + 1) % per_piece == 0:
            n = j // per_piece
            piece = pl.ds(n * per_piece * width, per_piece * width)
            send(
                None, far_send.at[:, piece], far_recv.at[:, piece], far_ss.at[n], far_rs.at[n], i, mate
            )
    for j in range(blocks):
        cols = pl.ds(pl.multiple_of(y * half + j * width, width), width)
        out_ref[:, cols] = (lat[own_rows, cols].astype(f32) + near[j]).astype(bf16)
    sent_all(wo.at[other_rows, pl.ds(0, strip)], wo_xss.at[0])
    sent_all(wo.at[other_rows, pl.ds(0, 2 * strip)], wo_tss.at[0])
    sent_all(ho.at[pl.ds(0, T - 1)], ho_ss.at[0])
    for n in range(FAR_PIECES):
        piece = pl.ds(n * per_piece * width, per_piece * width)
        arrived(far_recv.at[:, piece], far_ss.at[n], far_rs.at[n])
        for j in range(n * per_piece, (n + 1) * per_piece):
            cols = pl.ds(pl.multiple_of((1 - y) * half + j * width, width), width)
            out_ref[:, cols] = (
                lat[own_rows, cols].astype(f32)
                + far_recv[:, j * width : (j + 1) * width].astype(f32)
            ).astype(bf16)

    drain()


def fused_shards(S, T, *args):
    (latents, context, condition, context_condition, norm_gain, shift_weight, scale_weight,
     gate_weight, query_weight, key_weight, value_weight, subtract_share, head_gain,
     output_weight) = args
    rows, D = latents.shape
    crows = context.shape[0]
    count = rows * T
    Z = T // 2
    bf16, f32 = jnp.bfloat16, jnp.float32
    vmem = pl.BlockSpec(memory_space=pltpu.VMEM)
    hbm = pl.BlockSpec(memory_space=pltpu.HBM)
    dma = pltpu.SemaphoreType.DMA
    return pl.pallas_call(
        functools.partial(fused_kernel, S=S, T=T),
        out_shape=jax.ShapeDtypeStruct((rows, D), bf16),
        in_specs=[hbm] * 14,
        out_specs=vmem,
        scratch_shapes=[
            pltpu.VMEM((crows, D), bf16),
            pltpu.VMEM((1, condition.shape[0]), f32),
            pltpu.VMEM((1, condition.shape[0]), f32),
            pltpu.VMEM((1, D), f32),
            pltpu.VMEM((1, 1), f32),
            pltpu.VMEM((1, VALUE), f32),
            pltpu.VMEM((count, D), bf16),
            pltpu.VMEM((count // 2, D), bf16),
            pltpu.VMEM((crows, D), bf16),
            pltpu.VMEM((D, 3 * VALUE), bf16),
            pltpu.VMEM((T * VALUE, D // 2), bf16),
            pltpu.VMEM((VALUE, D // (2 * S)), bf16),
            pltpu.VMEM((S, 8, D // T), f32),
            pltpu.VMEM((T, 8, D // T), f32),
            pltpu.VMEM((2, count, VALUE), f32),
            pltpu.VMEM((2 * count, VALUE), bf16),
            pltpu.VMEM((S, count + crows, 2 * VALUE), bf16),
            pltpu.VMEM((count, VALUE), bf16),
            pltpu.VMEM((T, 2 * rows, VALUE), bf16),
            pltpu.VMEM(shift_weight.shape, bf16),
            pltpu.VMEM(shift_weight.shape, bf16),
            pltpu.VMEM(shift_weight.shape, bf16),
            pltpu.VMEM((rows, D // 2), bf16),
            pltpu.VMEM((rows, D // 2), bf16),
            pltpu.VMEM((2 * rows, D // 2), f32),
            pltpu.VMEM((2 * rows, 2 * VALUE), bf16),
            dma((16,)), dma((CHUNKS, 4)), dma((CHUNKS, Z + 1)), dma((CHUNKS,)), dma((1,)), dma((2,)),
            dma((1,)), dma((1,)), dma((1,)), dma((1,)), pltpu.SemaphoreType.REGULAR((3,)),
            dma((2, 3)), dma((2, S)), dma((3,)), dma((S,)),
            dma((1,)), dma((1,)), dma((1,)), dma((1,)), dma((T,)), dma((1,)), dma((T,)), dma((1,)), dma((2,)),
            dma((FAR_PIECES,)), dma((FAR_PIECES,)),
        ],
        compiler_params=pltpu.CompilerParams(
            collective_id=0, has_side_effects=True, vmem_limit_bytes=VMEM_LIMIT
        ),
    )(latents, context, condition[None, :], context_condition[None, :], norm_gain[None, :],
      shift_weight, scale_weight, gate_weight, query_weight, key_weight, value_weight,
      subtract_share[None, :], head_gain[None, :], output_weight)


def fits(S, T, shapes):
    rows = shapes[0][0] // (S * T)
    crows = shapes[1][0] // S
    D = shapes[0][1]
    heads = shapes[8][1] // VALUE
    return (
        S == 4 and T == 8 and heads == T and rows % 32 == 0
        and crows % 16 == 0 and D % (128 * T) == 0 and D % (128 * CHUNKS) == 0
        and rows * T * D * 8 + T * VALUE * D * 2 < 24 * 1024 * 1024
    )


def solution(mesh):
    in_specs = (
        P(("sp", "tp"), None),
        P("sp", None),
        P("sp"),
        P("sp"),
        P(),
        P("sp", "tp"),
        P("sp", "tp"),
        P("sp", "tp"),
        P(None, "tp"),
        P(None, "tp"),
        P(None, "tp"),
        P("tp"),
        P(),
        P("tp", None),
    )
    out_specs = P(("sp", "tp"), None)
    S, T = mesh.shape["sp"], mesh.shape["tp"]

    def whole(*args):
        if fits(S, T, [a.shape for a in args]):
            body = functools.partial(fused_shards, S, T)
        else:
            body = shards
        return jax.shard_map(
            body, mesh=mesh, in_specs=in_specs, out_specs=out_specs, check_vma=False
        )(*args)

    return whole
```
